32 devices in a mesh: fs: 16 (over z, y, x), tp: 2 (over core).
Axes of the slice: x: 2, y: 2, z: 4, core: 2. Of those that a mesh axis runs over, the one named last changes fastest.
Arguments:
- x_late: bfloat16 [3072, 2048], P(('fs', 'tp')), may hold values from -6 to 6
- x_early: bfloat16 [3072, 2048], P(('fs', 'tp')), may hold values from -6 to 6
- cotangent: bfloat16 [3072, 2048], P(('fs', 'tp')), may hold values from -0.3984375 to 0.3984375
- norm_gain: bfloat16 [2048], replicated, may hold values from 0.099609375 to 1.8984375
- gate_weight: bfloat16 [2048, 2816], P('fs', 'tp'), may hold values from -0.125 to 0.125
- up_weight: bfloat16 [2048, 2816], P('fs', 'tp'), may hold values from -0.125 to 0.125
- down_weight: bfloat16 [2048, 2816], P('fs', 'tp'), may hold values from -0.109375 to 0.109375
- gate_sum: float32 [2048, 2816], P('fs', 'tp'), may hold values from -6 to 6
- up_sum: float32 [2048, 2816], P('fs', 'tp'), may hold values from -6 to 6
- down_sum: float32 [2048, 2816], P('fs', 'tp'), may hold values from -6 to 6
Outputs:
- out_late: bfloat16 [3072, 2048], P(('fs', 'tp'))
- grad_early: bfloat16 [3072, 2048], P(('fs', 'tp'))
- gate_sum_out: float32 [2048, 2816], P('fs', 'tp')
- up_sum_out: float32 [2048, 2816], P('fs', 'tp')
- down_sum_out: float32 [2048, 2816], P('fs', 'tp')
The draws below stay inside these ranges and needn't reach their ends.
All inputs are finite; a program needn't handle non-finite values.
Results may differ from the reference program's by a relative error of at most 0.0095.
Values may be sent and summed in bfloat16 or wider, within the bound.
A program may use at most 128 MiB of HBM per device.

```python
import jax
import jax.numpy as jnp
from jax import lax

D = 2048
FF = 2816
TOKENS = 3072
N_TP = 2


def strengthened(array, key, source, target, shards_of, factor):
    owner, partner = [(jnp.arange(array.shape[dim]) // (array.shape[dim] // shards_of)).reshape([-1 if axis == dim else 1 for axis in range(array.ndim)]) for dim in (source, target)]
    chosen = jax.random.permutation(key, shards_of)[partner]
    strong = (owner == chosen) | (owner == (partner + shards_of // 2) % shards_of)
    return jnp.where(strong, factor * array, array)


def block_levels(key, dims, pieces, low, top_value):
    def one(axis_at, parts):
        heights = jax.random.uniform(jax.random.fold_in(jax.random.fold_in(key, 6), axis_at), (parts,), jnp.float32, low / len(pieces), top_value / len(pieces))
        return jnp.repeat(jnp.exp(heights), dims[axis_at] // parts).reshape((-1,) + (1,) * (len(dims) - axis_at - 1))

    loudness = one(*pieces[0])
    for cut in pieces[1:]:
        loudness = loudness * one(*cut)
    return loudness


def normal_values(rng, shape, deviation, reach, split=(), dtype=jnp.bfloat16):
    drawn = deviation * jax.random.normal(rng, shape, jnp.float32)
    if split:
        drawn = drawn * block_levels(rng, shape, split, -0.22, 0.18)
    return jnp.clip(drawn, -reach, reach).astype(dtype)


def noise_with(key, dims, scale, limit, pieces, heavy, kind=jnp.bfloat16):
    entries = scale * jax.random.normal(key, dims, jnp.float32)
    if pieces:
        entries = entries * block_levels(key, dims, pieces, -0.22, 0.18)
    return jnp.clip(strengthened(entries, jax.random.fold_in(key, 3), *heavy), -limit, limit).astype(kind)


def setup_inputs(seed: int = 0) -> dict:
    key_of = jax.random.split(jax.random.key(seed), 11)
    x_late = normal_values(key_of[0], (TOKENS, D), 1.0, 6.0, ((0, 32),))
    x_early = normal_values(key_of[1], (TOKENS, D), 1.0, 6.0, ((0, 32),))
    cotangent = noise_with(key_of[2], (TOKENS, D), 0.05, 0.3984375, ((0, 32),), (0, 1, 32, 2.75))
    norm_gain = jnp.clip(1.0 + 0.18 * jax.random.normal(key_of[3], (D,), jnp.float32), 0.099609375, 1.8984375).astype(jnp.bfloat16)
    gate_weight = normal_values(key_of[4], (D, FF), D ** -0.5, 0.125, ((0, 16), (1, 2)))
    up_weight = normal_values(key_of[5], (D, FF), D ** -0.5, 0.125, ((0, 16), (1, 2)))
    down_weight = normal_values(key_of[6], (D, FF), FF ** -0.5, 0.109375, ((0, 16), (1, 2)))
    gate_sum = normal_values(key_of[7], (D, FF), 1.0, 6.0, ((0, 16), (1, 2)), jnp.float32)
    up_sum = normal_values(key_of[8], (D, FF), 1.0, 6.0, ((0, 16), (1, 2)), jnp.float32)
    down_sum = normal_values(key_of[9], (D, FF), 1.0, 6.0, ((0, 16), (1, 2)), jnp.float32)
    return {"x_late": x_late, "x_early": x_early, "cotangent": cotangent, "norm_gain": norm_gain, "gate_weight": gate_weight, "up_weight": up_weight, "down_weight": down_weight, "gate_sum": gate_sum, "up_sum": up_sum, "down_sum": down_sum}


eps = 1e-06

def normalize(x, norm_gain):
    xf = x.astype(jnp.float32)
    inv = lax.rsqrt(lax.optimization_barrier(jnp.mean(xf * xf, axis=-1, keepdims=True)) + eps)
    return (xf, inv, (xf * inv * norm_gain.astype(jnp.float32)).astype(jnp.bfloat16))

def block_sum(pairs):
    width = FF // N_TP
    total = jnp.zeros((pairs[0][0].shape[0], pairs[0][1].shape[0]), jnp.float32)
    for block in range(N_TP):
        part = jnp.zeros_like(total)
        for left, right in pairs:
            part = part + jnp.dot(left[:, block * width:(block + 1) * width], right[:, block * width:(block + 1) * width].T, preferred_element_type=jnp.float32)
        rounded = lax.optimization_barrier(part.astype(jnp.bfloat16))
        total = total + rounded.astype(jnp.float32)
    return total

def reference(x_late, x_early, cotangent, norm_gain, gate_weight, up_weight, down_weight, gate_sum, up_sum, down_sum):
    late_f, late_inv, normed_late = normalize(x_late, norm_gain)
    gate_l = jnp.dot(normed_late, gate_weight, preferred_element_type=jnp.float32)
    up_l = jnp.dot(normed_late, up_weight, preferred_element_type=jnp.float32)
    hidden_l = (jax.nn.silu(gate_l) * up_l).astype(jnp.bfloat16)
    branch = block_sum([(hidden_l, down_weight)])
    out_late = (late_f + 0.5 * branch).astype(jnp.bfloat16)
    early_f, inv, normed_early = normalize(x_early, norm_gain)
    gate_e = jnp.dot(normed_early, gate_weight, preferred_element_type=jnp.float32)
    up_e = jnp.dot(normed_early, up_weight, preferred_element_type=jnp.float32)
    sig = jax.nn.sigmoid(gate_e)
    silu_e = gate_e * sig
    hidden_e = (silu_e * up_e).astype(jnp.bfloat16)
    half_cot = (0.5 * cotangent.astype(jnp.float32)).astype(jnp.bfloat16)
    down_grad = jnp.dot(half_cot.T, hidden_e, preferred_element_type=jnp.float32)
    d_hidden = jnp.dot(half_cot, down_weight, preferred_element_type=jnp.float32)
    d_gate = (d_hidden * up_e * sig * (1.0 + gate_e * (1.0 - sig))).astype(jnp.bfloat16)
    d_up = (d_hidden * silu_e).astype(jnp.bfloat16)
    gate_grad = jnp.dot(normed_early.T, d_gate, preferred_element_type=jnp.float32)
    up_grad = jnp.dot(normed_early.T, d_up, preferred_element_type=jnp.float32)
    d_normed = block_sum([(d_gate, gate_weight), (d_up, up_weight)])
    scaled = d_normed * norm_gain.astype(jnp.float32)
    d_input = inv * scaled - early_f * inv ** 3 * lax.optimization_barrier(jnp.mean(scaled * early_f, axis=-1, keepdims=True))
    grad_early = (cotangent.astype(jnp.float32) + d_input).astype(jnp.bfloat16)
    return (out_late, grad_early, gate_sum + gate_grad, up_sum + up_grad, down_sum + down_grad)
```

```python
import jax
import jax.numpy as jnp
from jax import lax
from jax.experimental import pallas as pl
from jax.experimental.pallas import tpu as pltpu
from jax.sharding import Mesh
from jax.sharding import PartitionSpec as P

eps = 1e-06


def normalize(x, gain):
    xf = x.astype(jnp.float32)
    inv = lax.rsqrt(jnp.mean(xf * xf, axis=-1, keepdims=True) + eps)
    return (inv, (xf * inv * gain).astype(jnp.bfloat16))


def contract_last(left, right):
    return lax.dot_general(
        left, right, (((1,), (1,)), ((), ())), preferred_element_type=jnp.float32
    )


def contract_first(left, right):
    return lax.dot_general(
        left, right, (((0,), (0,)), ((), ())), preferred_element_type=jnp.float32
    )


def dot(left, right):
    return jnp.dot(left, right, preferred_element_type=jnp.float32)


def make_on_device(split, n_tp):
    def shifted(value, axis, size, step):
        return lax.ppermute(value, axis, [(i, (i + step) % size) for i in range(size)])

    def gather_tokens(own):
        over_fi = [own] + [shifted(own, "fi", split, k) for k in range(1, split)]
        chip = jnp.concatenate(over_fi, axis=1)
        over_tp = [chip] + [shifted(chip, "tp", n_tp, j) for j in range(1, n_tp)]
        return jnp.concatenate(over_tp, axis=1)

    def scatter_tokens(part):
        blocks = part.astype(jnp.bfloat16).reshape((n_tp, split, -1, part.shape[-1]))
        mine = blocks[0].astype(jnp.float32)
        for j in range(1, n_tp):
            mine = mine + shifted(blocks[j], "tp", n_tp, -j).astype(jnp.float32)
        total = mine[0]
        if split > 1:
            sent = mine[1:].astype(jnp.bfloat16)
            for k in range(1, split):
                total = total + shifted(sent[k - 1], "fi", split, -k).astype(jnp.float32)
        return total

    def gather_weight(parts):
        rows, cols = parts[0].shape
        width = cols // split
        if split > 1:
            pieces = [p.reshape(rows, split, width).transpose(1, 0, 2) for p in parts]
            sent = jnp.concatenate(pieces, axis=2) if len(pieces) > 1 else pieces[0]
            sent = lax.all_to_all(sent, "fi", split_axis=0, concat_axis=0, tiled=True)
            sent = sent.reshape(split * rows, len(parts) * width)
        else:
            sent = jnp.concatenate(parts, axis=1) if len(parts) > 1 else parts[0]
        return lax.all_gather(sent, "fo", axis=0, tiled=True)

    def scatter_grad(grad, sums):
        rows, cols = sums[0].shape
        width = cols // split
        part = lax.psum_scatter(
            grad.astype(jnp.bfloat16), "fo", scatter_dimension=0, tiled=True
        )
        part = part.reshape(split, rows, len(sums) * width)
        if split > 1:
            part = lax.all_to_all(part, "fi", split_axis=0, concat_axis=0, tiled=True)
        outs = []
        for i, s in enumerate(sums):
            own = part[:, :, i * width : (i + 1) * width]
            own = own.transpose(1, 0, 2).reshape(rows, cols)
            outs.append(s + own.astype(jnp.float32))
        return outs

    def on_device(
        x_late,
        x_early,
        cotangent,
        norm_gain,
        gate_weight,
        up_weight,
        down_weight,
        gate_sum,
        up_sum,
        down_sum,
    ):
        width = gate_weight.shape[1] // split
        gain = norm_gain.astype(jnp.float32)
        inv_own, early_own = normalize(x_early, gain)
        _, late_own = normalize(x_late, gain)
        cot_own = (0.5 * cotangent.astype(jnp.float32)).astype(jnp.bfloat16)
        w_gu = gather_weight([gate_weight, up_weight])
        early_side = gather_tokens(jnp.stack([early_own, cot_own]))
        normed_early, half_cot = early_side[0], early_side[1]
        normed_late = gather_tokens(late_own[None])[0]
        w_down = gather_weight([down_weight])

        gu_e = dot(normed_early, w_gu)
        gate_e, up_e = gu_e[:, :width], gu_e[:, width:]
        sig = jax.nn.sigmoid(gate_e)
        silu_e = gate_e * sig
        hidden_e = (silu_e * up_e).astype(jnp.bfloat16)
        down_part = contract_first(half_cot, hidden_e)
        gu_l = dot(normed_late, w_gu)
        hidden_l = (jax.nn.silu(gu_l[:, :width]) * gu_l[:, width:]).astype(jnp.bfloat16)

        d_hidden = dot(half_cot, w_down)
        d_gate = (d_hidden * up_e * sig * (1.0 + gate_e * (1.0 - sig))).astype(jnp.bfloat16)
        d_up = (d_hidden * silu_e).astype(jnp.bfloat16)
        d_gu = jnp.concatenate([d_gate, d_up], axis=1)
        gu_part = contract_first(normed_early, d_gu)

        (down_out,) = scatter_grad(down_part, [down_sum])
        gate_out, up_out = scatter_grad(gu_part, [gate_sum, up_sum])

        d_normed = scatter_tokens(contract_last(d_gu, w_gu))
        branch = scatter_tokens(contract_last(hidden_l, w_down))
        out_late = (x_late.astype(jnp.float32) + 0.5 * branch).astype(jnp.bfloat16)
        early_f = x_early.astype(jnp.float32)
        scaled = d_normed * gain
        d_input = inv_own * scaled - early_f * inv_own**3 * jnp.mean(
            scaled * early_f, axis=-1, keepdims=True
        )
        grad_early = (cotangent.astype(jnp.float32) + d_input).astype(jnp.bfloat16)
        return (out_late, grad_early, gate_out, up_out, down_out)

    return on_device


MESH = pl.DeviceIdType.MESH
RING = 4
EARLY, COT, LATE = 0, 1, 2
GATE, UP, DOWN = 0, 1, 2
OWN, XN, YN, DIAG = 0, 1, 2, 3


def dot_nt(left, right):
    return lax.dot_general(
        left, right, (((1,), (1,)), ((), ())), preferred_element_type=jnp.float32
    )


def dot_tn(left, right):
    return lax.dot_general(
        left, right, (((0,), (0,)), ((), ())), preferred_element_type=jnp.float32
    )


class Net:
    def __init__(self, send_sems, recv_sems):
        self.send_sems, self.recv_sems, self.copies = send_sems, recv_sems, []

    def send(self, src, dst, device):
        i = len(self.copies)
        copy = pltpu.make_async_remote_copy(
            src_ref=src,
            dst_ref=dst,
            send_sem=self.send_sems.at[i],
            recv_sem=self.recv_sems.at[i],
            device_id=device,
            device_id_type=MESH,
        )
        copy.start()
        self.copies.append(copy)
        return copy


N_COPIES = 101


def step_kernel(
    wt, ne, co, la, dn_out, br_out, g_out,
    w, tok, gu, hid, dgu, hidl, gr, po, px_in, p_relay, p_dir, z_relay, z_dir, gs, gx,
    send_sems, recv_sems, local_sems,
):
    _, _, hidden, rows = wt.shape
    own_tokens, width = ne.shape
    tokens = tok.shape[1]
    half = own_tokens // 2
    z, p, c = lax.axis_index("fo"), lax.axis_index("fi"), lax.axis_index("tp")
    p_x, p_y, p_d = lax.rem(5 - p, 4), lax.rem(p + 2, 4), 3 - p
    z_n, z_p, z_o = lax.rem(z + 1, 4), lax.rem(z + 3, 4), lax.rem(z + 2, 4)
    to_x, to_y, to_d = {"fi": p_x}, {"fi": p_y}, {"fi": p_d}
    to_n, to_p, to_c = {"fo": z_n}, {"fo": z_p}, {"tp": 1 - c}

    barrier = pltpu.get_barrier_semaphore()
    partners = (to_x, to_y, to_d, to_n, to_p, to_c)
    for device in partners:
        pl.semaphore_signal(barrier, inc=1, device_id=device, device_id_type=MESH)
    pl.semaphore_wait(barrier, len(partners))

    net = Net(send_sems, recv_sems)
    groups = (slice(0, 2), slice(2, 3))
    GU, DN = 0, 1

    def lanes(zz, pp):
        return pl.ds(pl.multiple_of((zz * RING + pp) * rows, rows), rows)

    def slot(rel, r=1):
        return pl.ds((r * RING + rel) * own_tokens, own_tokens)

    def half_slot(rel, h, r=1):
        return pl.ds((r * RING + rel) * own_tokens + h * half, half)

    place = {"o": p, "x": p_x, "y": p_y, "d": p_d}
    toward = {"x": to_x, "y": to_y, "d": to_d}
    a2a, fwd, bwd = {}, {}, {}

    def spread(g, q):
        a2a[g, q] = net.send(
            wt.at[place[q], groups[g]], w.at[groups[g], :, lanes(z, p)], toward[q]
        )

    def along(g, q):
        block = w.at[groups[g], :, lanes(z, place[q])]
        src = wt.at[p, groups[g]] if q == "o" else block
        fwd[g, q] = net.send(src, block, to_n)
        bwd[g, q] = net.send(src, block, to_p)

    relay = {}

    def relay_on(g, q):
        if q in "od":
            fwd[g, q].wait_recv()
            block = w.at[groups[g], :, lanes(z_p, place[q])]
            relay[g, q] = net.send(block, block, to_n)
        else:
            bwd[g, q].wait_recv()
            block = w.at[groups[g], :, lanes(z_n, place[q])]
            relay[g, q] = net.send(block, block, to_p)

    own_in = (ne, co, la)
    tok_x, tok_y, tok_rx, tok_ry, tok_c = {}, {}, {}, {}, {}

    def own_half(a, axis, h):
        sent, rel, device = (tok_x, XN, to_x) if axis == "x" else (tok_y, YN, to_y)
        sent[a, h] = net.send(
            own_in[a].at[pl.ds(h * half, half)], tok.at[a, half_slot(rel, h)], device
        )

    def own_all(a):
        own_half(a, "x", 0)
        own_half(a, "y", 1)
        own_half(a, "x", 1)
        own_half(a, "y", 0)

    def relay_tokens(a):
        tok_x[a, 0].wait_recv()
        tok_rx[a] = net.send(
            tok.at[a, half_slot(XN, 0)], tok.at[a, half_slot(DIAG, 0)], to_y
        )
        tok_y[a, 1].wait_recv()
        tok_ry[a] = net.send(
            tok.at[a, half_slot(YN, 1)], tok.at[a, half_slot(DIAG, 1)], to_x
        )

    def pass_tokens(a, rel):
        src = own_in[a] if rel == OWN else tok.at[a, slot(rel)]
        tok_c[a, rel] = net.send(src, tok.at[a, slot(rel, 0)], to_c)

    def pass_near(a):
        tok_x[a, 1].wait_recv()
        pass_tokens(a, XN)
        tok_y[a, 0].wait_recv()
        pass_tokens(a, YN)

    def pass_far(a):
        tok_rx[a].wait_recv()
        tok_ry[a].wait_recv()
        pass_tokens(a, DIAG)

    def tokens_here(a):
        for rel in range(RING):
            tok_c[a, rel].wait_recv()

    along(GU, "o")
    for q in "xyd":
        spread(GU, q)
    own_all(EARLY)
    along(DN, "o")
    for q in "xyd":
        spread(DN, q)
    for a in range(3):
        pass_tokens(a, OWN)
    local = [pltpu.make_async_copy(wt.at[p], w.at[:, :, lanes(z, p)], local_sems.at[0])]
    for a in range(3):
        local.append(
            pltpu.make_async_copy(own_in[a], tok.at[a, slot(OWN)], local_sems.at[1 + a])
        )
    for copy in local:
        copy.start()

    def arrived(g, q):
        a2a[g, q].wait_recv()
        along(g, q)

    arrived(GU, "x")
    arrived(GU, "y")
    relay_on(GU, "o")
    arrived(GU, "d")
    relay_on(GU, "x")
    relay_tokens(EARLY)
    own_all(COT)
    relay_on(GU, "y")
    pass_near(EARLY)
    arrived(DN, "x")
    arrived(DN, "y")
    arrived(DN, "d")
    relay_on(GU, "d")
    relay_on(DN, "o")
    relay_on(DN, "x")
    relay_on(DN, "y")
    pass_far(EARLY)
    for copy in local:
        copy.wait()

    def weights_here(g):
        for q in "xy":
            fwd[g, q].wait_recv()
        for q in "od":
            bwd[g, q].wait_recv()
        for q in "oxyd":
            relay[g, q].wait_recv()

    weights_here(GU)
    tokens_here(EARLY)

    chunk = 2 * 128
    n_chunks = tokens // chunk

    def chunk_of(n):
        return pl.ds(pl.multiple_of(n * chunk, chunk), chunk)

    @pl.loop(0, n_chunks)
    def _(n):
        cols = chunk_of(n)
        x = tok[EARLY, cols, :]
        gate, up = dot_nt(w[GATE], x), dot_nt(w[UP], x)
        gu[0, :, cols] = gate
        gu[1, :, cols] = up
        hid[:, cols] = (gate * jax.nn.sigmoid(gate) * up).astype(jnp.bfloat16)

    relay_tokens(COT)
    own_all(LATE)
    pass_near(COT)
    relay_on(DN, "d")
    pass_far(COT)
    tokens_here(COT)

    span = RING * rows
    pair = span // 2
    left, right = pl.ds(0, pair), pl.ds(pair, pair)

    def span_of(n):
        return pl.ds(pl.multiple_of(n * span, span), span)

    rs = {}

    def grad_out(m):
        rs[m, "rn"] = net.send(gr.at[m, z_o, :, left], z_relay.at[0, m], to_n)
        rs[m, "rp"] = net.send(gr.at[m, z_o, :, right], z_relay.at[1, m], to_p)
        rs[m, "n1"] = net.send(gr.at[m, z_n, :, right], z_dir.at[0, m, :, right], to_n)
        rs[m, "p0"] = net.send(gr.at[m, z_p, :, left], z_dir.at[1, m, :, left], to_p)

    def add_to(ref, index, term):
        ref[index] = (ref[index].astype(jnp.float32) + term.astype(jnp.float32)).astype(
            jnp.bfloat16
        )

    def grad_relay(m):
        rs[m, "rn"].wait_recv()
        add_to(gr, (m, z_n, slice(None), left), z_relay[0, m])
        rs[m, "n0"] = net.send(gr.at[m, z_n, :, left], z_dir.at[0, m, :, left], to_n)
        rs[m, "rp"].wait_recv()
        add_to(gr, (m, z_p, slice(None), right), z_relay[1, m])
        rs[m, "p1"] = net.send(gr.at[m, z_p, :, right], z_dir.at[1, m, :, right], to_p)

    def grad_final(m):
        for k in ("n0", "n1", "p0", "p1"):
            rs[m, k].wait_recv()
        total = gr[m, z].astype(jnp.float32)
        total = total + z_dir[0, m].astype(jnp.float32) + z_dir[1, m].astype(jnp.float32)
        total = total.astype(jnp.bfloat16)
        for k in range(RING):
            gs[m, k] = total[:, k * rows : (k + 1) * rows]
        for q in "xyd":
            rs[m, q] = net.send(gs.at[m, place[q]], gx.at[p, m], toward[q])
        gx[p, m] = gs[m, p]

    @pl.loop(0, RING)
    def _(n):
        gr[DOWN, n] = jnp.dot(
            hid[...], tok[COT, :, span_of(n)], preferred_element_type=jnp.float32
        ).astype(jnp.bfloat16)

    grad_out(DOWN)
    weights_here(DN)

    @pl.loop(0, n_chunks)
    def _(n):
        cols = chunk_of(n)
        d_hidden = dot_nt(w[DOWN], tok[COT, cols, :])
        gate, up = gu[0, :, cols], gu[1, :, cols]
        sig = jax.nn.sigmoid(gate)
        dgu[0, :, cols] = (d_hidden * up * sig * (1.0 + gate * (1.0 - sig))).astype(
            jnp.bfloat16
        )
        dgu[1, :, cols] = (d_hidden * (gate * sig)).astype(jnp.bfloat16)

    for m in (GATE, UP):

        @pl.loop(0, RING)
        def _(n, m=m):
            gr[m, n] = jnp.dot(
                dgu[m], tok[EARLY, :, span_of(n)], preferred_element_type=jnp.float32
            ).astype(jnp.bfloat16)

        grad_out(m)

    grad_relay(DOWN)
    relay_tokens(LATE)

    group = tokens // 2
    out = {}

    def partial(a, r, pairs):
        @pl.loop(0, width // span)
        def _(n):
            cols = span_of(n)
            acc = None
            for ref, index, m in pairs:
                term = dot_tn(ref[index + (slice(None), pl.ds(r * group, group))], w[m, :, cols])
                acc = term if acc is None else acc + term
            po[a, pl.ds(r * group, group), cols] = acc.astype(jnp.bfloat16)

    def partial_both(a, pairs):
        partial(a, 0, pairs)
        out[a, "c"] = net.send(po.at[a, pl.ds(0, group)], px_in.at[a], to_c)
        partial(a, 1, pairs)

    def join_cores(a):
        out[a, "c"].wait_recv()
        @pl.loop(0, RING)
        def _(n):
            at = pl.ds(pl.multiple_of(n * own_tokens, own_tokens), own_tokens)
            at_po = pl.ds(pl.multiple_of(group + n * own_tokens, own_tokens), own_tokens)
            add_to(po, (a, at_po, slice(None)), px_in[a, at, :])

        top, bottom = pl.ds(0, half), pl.ds(half, half)
        out[a, "rx"] = net.send(po.at[a, half_slot(DIAG, 0)], p_relay.at[a, 0], to_x)
        out[a, "ry"] = net.send(po.at[a, half_slot(DIAG, 1)], p_relay.at[a, 1], to_y)
        out[a, "x0"] = net.send(po.at[a, half_slot(XN, 0)], p_dir.at[a, 0, top], to_x)
        out[a, "y1"] = net.send(po.at[a, half_slot(YN, 1)], p_dir.at[a, 1, bottom], to_y)

    def out_relay(a):
        top, bottom = pl.ds(0, half), pl.ds(half, half)
        out[a, "rx"].wait_recv()
        add_to(po, (a, half_slot(YN, 0), slice(None)), p_relay[a, 0])
        out[a, "y0"] = net.send(po.at[a, half_slot(YN, 0)], p_dir.at[a, 1, top], to_y)
        out[a, "ry"].wait_recv()
        add_to(po, (a, half_slot(XN, 1), slice(None)), p_relay[a, 1])
        out[a, "x1"] = net.send(po.at[a, half_slot(XN, 1)], p_dir.at[a, 0, bottom], to_x)

    def out_final(a, ref):
        for k in ("x0", "x1", "y0", "y1"):
            out[a, k].wait_recv()
        ref[...] = (
            po[a, slot(OWN), :].astype(jnp.float32)
            + p_dir[a, 0].astype(jnp.float32)
            + p_dir[a, 1].astype(jnp.float32)
        )

    partial_both(0, ((dgu, (0,), GATE), (dgu, (1,), UP)))
    grad_relay(GATE)
    pass_near(LATE)
    join_cores(0)
    grad_relay(UP)
    pass_far(LATE)
    tokens_here(LATE)

    @pl.loop(0, n_chunks)
    def _(n):
        cols = chunk_of(n)
        x = tok[LATE, cols, :]
        gate, up = dot_nt(w[GATE], x), dot_nt(w[UP], x)
        hidl[:, cols] = (gate * jax.nn.sigmoid(gate) * up).astype(jnp.bfloat16)

    grad_final(DOWN)
    partial_both(1, ((hidl, (), DOWN),))
    out_relay(0)
    join_cores(1)
    grad_final(GATE)
    out_relay(1)
    grad_final(UP)
    out_final(0, dn_out)
    out_final(1, br_out)
    for m in (DOWN, GATE, UP):
        for q in "xyd":
            rs[m, q].wait_recv()
    g_out[...] = gx[...]
    assert len(net.copies) == N_COPIES
    for copy in net.copies:
        copy.wait_send()


def run_step(wt, ne, co, la):
    _, _, hidden, rows = wt.shape
    own, width = ne.shape
    tokens = 2 * RING * own
    bf16, f32 = jnp.bfloat16, jnp.float32
    span = RING * rows
    vmem = pltpu.VMEM
    return pl.pallas_call(
        step_kernel,
        out_shape=(
            jax.ShapeDtypeStruct((own, width), f32),
            jax.ShapeDtypeStruct((own, width), f32),
            jax.ShapeDtypeStruct(wt.shape, bf16),
        ),
        in_specs=[pl.BlockSpec(memory_space=pltpu.VMEM)] * 4,
        out_specs=[pl.BlockSpec(memory_space=pltpu.VMEM)] * 3,
        scratch_shapes=[
            vmem((3, hidden, width), bf16),
            vmem((3, tokens, width), bf16),
            vmem((2, hidden, tokens), f32),
            vmem((hidden, tokens), bf16),
            vmem((2, hidden, tokens), bf16),
            vmem((hidden, tokens), bf16),
            vmem((3, RING, hidden, span), bf16),
            vmem((2, tokens, width), bf16),
            vmem((2, tokens // 2, width), bf16),
            vmem((2, 2, own // 2, width), bf16),
            vmem((2, 2, own, width), bf16),
            vmem((2, 3, hidden, span // 2), bf16),
            vmem((2, 3, hidden, span), bf16),
            vmem((3, RING, hidden, rows), bf16),
            vmem((RING, 3, hidden, rows), bf16),
            pltpu.SemaphoreType.DMA((N_COPIES,)),
            pltpu.SemaphoreType.DMA((N_COPIES,)),
            pltpu.SemaphoreType.DMA((4,)),
        ],
        compiler_params=pltpu.CompilerParams(
            collective_id=0, has_side_effects=True, vmem_limit_bytes=60 * 2**20
        ),
        name="step",
    )(wt, ne, co, la)


def on_device_rings(
    x_late, x_early, cotangent, norm_gain,
    gate_weight, up_weight, down_weight, gate_sum, up_sum, down_sum,
):
    gain = norm_gain.astype(jnp.float32)
    inv_own, early_own = normalize(x_early, gain)
    _, late_own = normalize(x_late, gain)
    cot_own = (0.5 * cotangent.astype(jnp.float32)).astype(jnp.bfloat16)
    rows, cols = gate_weight.shape
    stacked = jnp.stack([gate_weight, up_weight, down_weight])
    wt = stacked.reshape(3, rows, RING, cols // RING).transpose(2, 0, 3, 1)
    d_normed, branch, grads = run_step(wt, early_own, cot_own, late_own)
    grads = grads.transpose(1, 3, 0, 2).reshape(3, rows, cols).astype(jnp.float32)
    out_late = (x_late.astype(jnp.float32) + 0.5 * branch).astype(jnp.bfloat16)
    early_f = x_early.astype(jnp.float32)
    scaled = d_normed * gain
    d_input = inv_own * scaled - early_f * inv_own**3 * jnp.mean(
        scaled * early_f, axis=-1, keepdims=True
    )
    grad_early = (cotangent.astype(jnp.float32) + d_input).astype(jnp.bfloat16)
    return (
        out_late,
        grad_early,
        gate_sum + grads[0],
        up_sum + grads[1],
        down_sum + grads[2],
    )


WANTED = 8


def solution(mesh):
    n_fs, n_tp = mesh.shape["fs"], mesh.shape["tp"]
    split = max(1, WANTED // n_tp)
    while n_fs % split:
        split //= 2
    fine = Mesh(mesh.devices.reshape(n_fs // split, split, n_tp), ("fo", "fi", "tp"))
    tokens, rows = P(("fo", "fi", "tp"), None), P(("fo", "fi"), "tp")
    rings = n_tp == 2 and split == RING and n_fs // split == RING
    return jax.shard_map(
        on_device_rings if rings else make_on_device(split, n_tp),
        mesh=fine,
        in_specs=(tokens, tokens, tokens, P()) + (rows,) * 6,
        out_specs=(tokens, tokens, rows, rows, rows),
        check_vma=False,
    )
```

```python
import jax
import jax.numpy as jnp
from jax import lax
from jax.experimental import pallas as pl
from jax.experimental.pallas import tpu as pltpu
from jax.sharding import Mesh
from jax.sharding import PartitionSpec as P

eps = 1e-06


def normalize(x, gain):
    xf = x.astype(jnp.float32)
    inv = lax.rsqrt(jnp.mean(xf * xf, axis=-1, keepdims=True) + eps)
    return (inv, (xf * inv * gain).astype(jnp.bfloat16))


def contract_last(left, right):
    return lax.dot_general(
        left, right, (((1,), (1,)), ((), ())), preferred_element_type=jnp.float32
    )


def contract_first(left, right):
    return lax.dot_general(
        left, right, (((0,), (0,)), ((), ())), preferred_element_type=jnp.float32
    )


def dot(left, right):
    return jnp.dot(left, right, preferred_element_type=jnp.float32)


def make_on_device(split, n_tp):
    def shifted(value, axis, size, step):
        return lax.ppermute(value, axis, [(i, (i + step) % size) for i in range(size)])

    def gather_tokens(own):
        over_fi = [own] + [shifted(own, "fi", split, k) for k in range(1, split)]
        chip = jnp.concatenate(over_fi, axis=1)
        over_tp = [chip] + [shifted(chip, "tp", n_tp, j) for j in range(1, n_tp)]
        return jnp.concatenate(over_tp, axis=1)

    def scatter_tokens(part):
        blocks = part.astype(jnp.bfloat16).reshape((n_tp, split, -1, part.shape[-1]))
        mine = blocks[0].astype(jnp.float32)
        for j in range(1, n_tp):
            mine = mine + shifted(blocks[j], "tp", n_tp, -j).astype(jnp.float32)
        total = mine[0]
        if split > 1:
            sent = mine[1:].astype(jnp.bfloat16)
            for k in range(1, split):
                total = total + shifted(sent[k - 1], "fi", split, -k).astype(jnp.float32)
        return total

    def gather_weight(parts):
        rows, cols = parts[0].shape
        width = cols // split
        if split > 1:
            pieces = [p.reshape(rows, split, width).transpose(1, 0, 2) for p in parts]
            sent = jnp.concatenate(pieces, axis=2) if len(pieces) > 1 else pieces[0]
            sent = lax.all_to_all(sent, "fi", split_axis=0, concat_axis=0, tiled=True)
            sent = sent.reshape(split * rows, len(parts) * width)
        else:
            sent = jnp.concatenate(parts, axis=1) if len(parts) > 1 else parts[0]
        return lax.all_gather(sent, "fo", axis=0, tiled=True)

    def scatter_grad(grad, sums):
        rows, cols = sums[0].shape
        width = cols // split
        part = lax.psum_scatter(
            grad.astype(jnp.bfloat16), "fo", scatter_dimension=0, tiled=True
        )
        part = part.reshape(split, rows, len(sums) * width)
        if split > 1:
            part = lax.all_to_all(part, "fi", split_axis=0, concat_axis=0, tiled=True)
        outs = []
        for i, s in enumerate(sums):
            own = part[:, :, i * width : (i + 1) * width]
            own = own.transpose(1, 0, 2).reshape(rows, cols)
            outs.append(s + own.astype(jnp.float32))
        return outs

    def on_device(
        x_late,
        x_early,
        cotangent,
        norm_gain,
        gate_weight,
        up_weight,
        down_weight,
        gate_sum,
        up_sum,
        down_sum,
    ):
        width = gate_weight.shape[1] // split
        gain = norm_gain.astype(jnp.float32)
        inv_own, early_own = normalize(x_early, gain)
        _, late_own = normalize(x_late, gain)
        cot_own = (0.5 * cotangent.astype(jnp.float32)).astype(jnp.bfloat16)
        w_gu = gather_weight([gate_weight, up_weight])
        early_side = gather_tokens(jnp.stack([early_own, cot_own]))
        normed_early, half_cot = early_side[0], early_side[1]
        normed_late = gather_tokens(late_own[None])[0]
        w_down = gather_weight([down_weight])

        gu_e = dot(normed_early, w_gu)
        gate_e, up_e = gu_e[:, :width], gu_e[:, width:]
        sig = jax.nn.sigmoid(gate_e)
        silu_e = gate_e * sig
        hidden_e = (silu_e * up_e).astype(jnp.bfloat16)
        down_part = contract_first(half_cot, hidden_e)
        gu_l = dot(normed_late, w_gu)
        hidden_l = (jax.nn.silu(gu_l[:, :width]) * gu_l[:, width:]).astype(jnp.bfloat16)

        d_hidden = dot(half_cot, w_down)
        d_gate = (d_hidden * up_e * sig * (1.0 + gate_e * (1.0 - sig))).astype(jnp.bfloat16)
        d_up = (d_hidden * silu_e).astype(jnp.bfloat16)
        d_gu = jnp.concatenate([d_gate, d_up], axis=1)
        gu_part = contract_first(normed_early, d_gu)

        (down_out,) = scatter_grad(down_part, [down_sum])
        gate_out, up_out = scatter_grad(gu_part, [gate_sum, up_sum])

        d_normed = scatter_tokens(contract_last(d_gu, w_gu))
        branch = scatter_tokens(contract_last(hidden_l, w_down))
        out_late = (x_late.astype(jnp.float32) + 0.5 * branch).astype(jnp.bfloat16)
        early_f = x_early.astype(jnp.float32)
        scaled = d_normed * gain
        d_input = inv_own * scaled - early_f * inv_own**3 * jnp.mean(
            scaled * early_f, axis=-1, keepdims=True
        )
        grad_early = (cotangent.astype(jnp.float32) + d_input).astype(jnp.bfloat16)
        return (out_late, grad_early, gate_out, up_out, down_out)

    return on_device


MESH = pl.DeviceIdType.MESH
PARTS = 2
GROUP = 4
EARLY, COT, LATE = 0, 1, 2
GATE, UP, DOWN = 0, 1, 2
OWN, ZN, YN, DIAG = 0, 1, 2, 3


def dot_nt(left, right):
    return lax.dot_general(
        left, right, (((1,), (1,)), ((), ())), preferred_element_type=jnp.float32
    )


def dot_tn(left, right):
    return lax.dot_general(
        left, right, (((0,), (0,)), ((), ())), preferred_element_type=jnp.float32
    )


class Net:
    def __init__(self, send_sems, recv_sems):
        self.send_sems, self.recv_sems, self.copies = send_sems, recv_sems, {}

    def plan(self, name, src, dst, device):
        i = len(self.copies)
        self.copies[name] = pltpu.make_async_remote_copy(
            src_ref=src,
            dst_ref=dst,
            send_sem=self.send_sems.at[i],
            recv_sem=self.recv_sems.at[i],
            device_id=device,
            device_id_type=MESH,
        )

    def start(self, *name):
        self.copies[name].start()

    def recv(self, *name):
        self.copies[name].wait_recv()


N_COPIES = 114


def step_kernel(
    wt, x_late, x_early, cotangent, norm_gain, late_out, early_out, g_out,
    w, tok, hid, dgu, hidl, gr, po, px_in, o_relay, o_dir, g_relay, g_dir, gs, gx,
    gwa, gwb,
    send_sems, recv_sems, local_sems,
):
    _, n_parts, _, part, rows = wt.shape
    own_tokens, width = x_early.shape
    tokens = tok.shape[1]
    half = own_tokens // 2
    zh, zi = lax.axis_index("zh"), lax.axis_index("zi")
    y, x, c = lax.axis_index("y"), lax.axis_index("x"), lax.axis_index("tp")
    inner = lax.rem(zh + zi, 2)
    is_inner, is_outer = inner == 1, inner == 0
    to_x, to_y, to_z = {"x": 1 - x}, {"y": 1 - y}, {"zi": 1 - zi}
    to_d, to_c = {"zi": 1 - zi, "y": 1 - y}, {"tp": 1 - c}
    to_m = {"zh": 1 - zh, "zi": 1 - zi}

    barrier = pltpu.get_barrier_semaphore()
    partners = (to_x, to_y, to_z, to_d, to_m, to_c)
    for device in partners:
        pl.semaphore_signal(barrier, inc=1, device_id=device, device_id_type=MESH)

    def own_rows(a):
        return tok.at[a, pl.ds((GROUP + OWN) * own_tokens, own_tokens)]

    gain = norm_gain[...].astype(jnp.float32)
    own_rows(EARLY)[...] = normalize(x_early[...], gain)[1]
    own_rows(COT)[...] = (0.5 * cotangent[...].astype(jnp.float32)).astype(jnp.bfloat16)
    own_rows(LATE)[...] = normalize(x_late[...], gain)[1]
    pl.semaphore_wait(barrier, len(partners))

    net = Net(send_sems, recv_sems)
    start, recv, plan = net.start, net.recv, net.plan
    A, B = 0, 1
    seats = {"o": (inner, y), "y": (inner, 1 - y), "z": (1 - inner, y), "d": (1 - inner, 1 - y)}
    toward = {"y": to_y, "z": to_z, "d": to_d}

    def seat(q):
        return seats[q][0] * 2 + seats[q][1]

    def lanes(zh_, in_, y_, x_):
        z_ = in_ + zh_ * (3 - 2 * in_)
        return pl.ds(pl.multiple_of(((z_ * 2 + y_) * 2 + x_) * rows, rows), rows)

    def slot(rel, r=1):
        return pl.ds((r * GROUP + rel) * own_tokens, own_tokens)

    def half_slot(rel, h, r=1):
        return pl.ds((r * GROUP + rel) * own_tokens + h * half, half)

    for g in range(n_parts):
        for q in "yzd":
            plan(("a", g, q), wt.at[seat(q), g], w.at[g, :, :, lanes(zh, *seats["o"], x)], toward[q])
        for i, q in enumerate("oyzd"):
            block = w.at[g, :, :, lanes(zh, *seats[q], x)]
            src = wt.at[seat("o"), g] if q == "o" else block
            plan(("h", g, q), src, block, to_m)
            far = w.at[g, :, :, lanes(1 - zh, *seats[q], x)]
            if g == A:
                outer_seat = (1 - seats[q][0], seats[q][1])
                outer_far = w.at[g, :, :, lanes(1 - zh, *outer_seat, x)]
                plan(("ga", g, q), src, gwa.at[i], to_z)
                plan(("gb", g, q), gwa.at[i], gwb.at[i], to_m)
                plan(("gc", g, q), gwb.at[i], outer_far, to_z)
            plan(("x", g, q), src, block, to_x)
            plan(("xr", g, q), far, far, to_x)
        for k in range(GROUP):
            mine = gr.at[g, 1 - zh, x, k]
            plan(("gr", g, k), gr.at[g, 1 - zh, 1 - x, k], g_relay.at[g, k], to_x)
            plan(("gx", g, k), gr.at[g, zh, 1 - x, k], g_dir.at[g, 0, k], to_x)
            plan(("gh", g, k), mine, g_dir.at[g, 1, k], to_m)
        for q in "dzy":
            plan(("gf", g, q), gs.at[g, seat(q)], gx.at[seat("o"), g], toward[q])
    for a in range(3):
        for h in range(2):
            src = tok.at[a, half_slot(OWN, h)]
            plan(("tz", a, h), src, tok.at[a, half_slot(ZN, h)], to_z)
            plan(("ty", a, h), src, tok.at[a, half_slot(YN, h)], to_y)
            plan(("tr", a, h), tok.at[a, half_slot(ZN, h)], tok.at[a, half_slot(DIAG, h)], to_y)
        for rel in range(GROUP):
            plan(("tc", a, rel), tok.at[a, slot(rel)], tok.at[a, slot(rel, 0)], to_c)
    for a in range(2):
        plan(("oc", a), po.at[a, pl.ds(0, GROUP * own_tokens)], px_in.at[a], to_c)
        plan(("oy", a), po.at[a, slot(YN)], o_dir.at[a, 0], to_y)
        for h in range(2):
            plan(("od", a, h), po.at[a, half_slot(DIAG, h)], o_relay.at[a, h], to_y)
            to_half = o_dir.at[a, 1, pl.ds(h * half, half)]
            plan(("oz", a, h), po.at[a, half_slot(ZN, h)], to_half, to_z)

    def spread(g, q):
        start("a", g, q)

    def along(g, q, role):
        start("ga" if g == A and not role else "h", g, q)
        start("x", g, q)

    def arrived(g, q, role):
        recv("a", g, q)
        along(g, q, role)

    def relay_on(g, q, role):
        recv("gc" if g == A and not role else "h", g, q)
        start("xr", g, q)

    def pass1(g, *some):
        for q in some:
            recv("ga", g, q)
            start("gb", g, q)

    def pass2(g, *some):
        for q in some:
            recv("gb", g, q)
            start("gc", g, q)

    def weights_here(g):
        for q in "oyzd":
            recv("x", g, q)
            recv("xr", g, q)

    def own_half(a, h):
        start("tz", a, h)
        start("ty", a, h)

    def own_all(a):
        own_half(a, 0)
        own_half(a, 1)

    def relay_half(a, h):
        recv("tz", a, h)
        start("tr", a, h)
        if h == 1:
            start("tc", a, ZN)

    def relay_tokens(a):
        relay_half(a, 0)
        relay_half(a, 1)

    def pass_near(a):
        for h in range(2):
            recv("ty", a, h)
        start("tc", a, YN)

    def pass_far(a):
        for h in range(2):
            recv("tr", a, h)
        start("tc", a, DIAG)

    def tokens_here(a):
        for rel in range(GROUP):
            recv("tc", a, rel)

    chunk = 2 * 128
    n_chunks = tokens // chunk
    span = 4 * rows
    group = tokens // 2

    def chunk_of(n):
        return pl.ds(pl.multiple_of(n * chunk, chunk), chunk)

    def span_of(n):
        return pl.ds(pl.multiple_of(n * span, span), span)

    def merged(ref):
        value = ref[...]
        return value.reshape(value.shape[0] * value.shape[1], value.shape[2])

    def gate_up(g, rows_in):
        both = dot_nt(merged(w.at[g, pl.ds(0, 2)]), rows_in)
        return both[:part], both[part:]

    def early(g):
        @pl.loop(0, n_chunks)
        def _(n):
            cols = chunk_of(n)
            gate, up = gate_up(g, tok[EARLY, cols, :])
            d_hidden = dot_nt(w[g, DOWN], tok[COT, cols, :])
            sig = jax.nn.sigmoid(gate)
            silu = gate * sig
            hid[g, :, cols] = (silu * up).astype(jnp.bfloat16)
            d_gate = d_hidden * up * sig * (1.0 + gate * (1.0 - sig))
            dgu[g, pl.ds(0, part), cols] = d_gate.astype(jnp.bfloat16)
            dgu[g, pl.ds(part, part), cols] = (d_hidden * silu).astype(jnp.bfloat16)

    def weight_grads(g):
        @pl.loop(0, width // span)
        def _(n):
            cols = span_of(n)
            for at, left, a in ((0, dgu, EARLY), (2 * part, hid, COT)):
                grad = jnp.dot(
                    left[g], tok[a, :, cols], preferred_element_type=jnp.float32
                ).astype(jnp.bfloat16)
                for yy in range(2):
                    for xx in range(2):
                        k = (yy * 2 + xx) * rows
                        gr[g, n // 2, xx, ((n + n // 2) % 2) * 2 + yy, pl.ds(at, grad.shape[0])] = (
                            grad[:, k : k + rows]
                        )

    def late():
        @pl.loop(0, n_chunks)
        def _(n):
            cols = chunk_of(n)
            for g in range(n_parts):
                gate, up = gate_up(g, tok[LATE, cols, :])
                hidl[g, :, cols] = (gate * jax.nn.sigmoid(gate) * up).astype(jnp.bfloat16)

    def add_to(ref, index, term):
        ref[index] = (ref[index].astype(jnp.float32) + term.astype(jnp.float32)).astype(
            jnp.bfloat16
        )

    def grad_far(g):
        for k in range(GROUP):
            start("gr", g, k)

    def grad_near(g, *some):
        for k in some:
            start("gx", g, k)

    def grad_relay(g, *some):
        for k in some:
            recv("gr", g, k)
            add_to(gr, (g, 1 - zh, x, k), g_relay[g, k])
            start("gh", g, k)

    def grad_final(g):
        for k in range(GROUP):
            recv("gh", g, k)
        for k in range(GROUP):
            recv("gx", g, k)
            total = gr[g, zh, x, k].astype(jnp.float32)
            total = total + g_dir[g, 0, k].astype(jnp.float32)
            total = total + g_dir[g, 1, k].astype(jnp.float32)
            gs[g, k] = total.astype(jnp.bfloat16)
        for q in "dzy":
            start("gf", g, q)
        gx[seat("o"), g] = gs[g, seat("o")]

    def grad_done(g):
        for q in "dzy":
            recv("gf", g, q)

    def partial(a, r, pairs):
        @pl.loop(0, width // span)
        def _(n):
            cols = span_of(n)
            acc = None
            for g in range(n_parts):
                for ref, height, m in pairs:
                    left = ref[g, :, pl.ds(r * group, group)]
                    right = merged(w.at[g, pl.ds(m, height), :, cols])
                    term = dot_tn(left, right)
                    acc = term if acc is None else acc + term
            po[a, pl.ds(r * group, group), cols] = acc.astype(jnp.bfloat16)

    def partial_both(a, pairs):
        partial(a, 0, pairs)
        start("oc", a)
        partial(a, 1, pairs)

    def join_cores(a):
        recv("oc", a)

        @pl.loop(0, GROUP)
        def _(n):
            at = pl.ds(pl.multiple_of(n * own_tokens, own_tokens), own_tokens)
            at_po = pl.ds(pl.multiple_of(group + n * own_tokens, own_tokens), own_tokens)
            add_to(po, (a, at_po, slice(None)), px_in[a, at, :])

        for h in range(2):
            start("od", a, h)
        start("oy", a)

    def out_relay(a):
        for h in range(2):
            recv("od", a, h)
            add_to(po, (a, half_slot(ZN, h), slice(None)), o_relay[a, h])
            start("oz", a, h)

    def out_total(a):
        recv("oy", a)
        for h in range(2):
            recv("oz", a, h)
        return (
            po[a, slot(OWN), :].astype(jnp.float32)
            + o_dir[a, 0].astype(jnp.float32)
            + o_dir[a, 1].astype(jnp.float32)
        )

    def early_final():
        early_f = x_early[...].astype(jnp.float32)
        inv = normalize(early_f, gain)[0]
        scaled = out_total(0) * gain
        d_input = inv * scaled - early_f * inv**3 * jnp.mean(
            scaled * early_f, axis=-1, keepdims=True
        )
        early_out[...] = (cotangent[...].astype(jnp.float32) + d_input).astype(jnp.bfloat16)

    def late_final():
        late_f = x_late[...].astype(jnp.float32)
        late_out[...] = (late_f + 0.5 * out_total(1)).astype(jnp.bfloat16)

    def take_in(role):
        for q in "zdy":
            spread(A, q)
        along(A, "o", role)
        own_half(EARLY, 0)
        if role:
            own_half(EARLY, 1)
        arrived(A, "y", role)
        arrived(A, "z", role)
        arrived(A, "d", role)
        if role:
            own_all(COT)
            relay_on(A, "o", role)
            pass1(A, "o")
            relay_on(A, "y", role)
            relay_on(A, "z", role)
            relay_half(EARLY, 0)
            relay_on(A, "d", role)
            pass1(A, "y")
            pass2(A, "o")
            pass_near(EARLY)
            pass1(A, "z")
            pass2(A, "y")
            pass1(A, "d")
            along(B, "o", role)
            pass2(A, "z")
            relay_half(EARLY, 1)
            pass2(A, "d")
            spread(B, "z")
            pass_near(COT)
            relay_half(COT, 0)
            relay_half(COT, 1)
            spread(B, "d")
            spread(B, "y")
        else:
            own_half(EARLY, 1)
            own_all(COT)
            relay_half(EARLY, 0)
            relay_half(EARLY, 1)
            pass_near(EARLY)
            relay_half(COT, 0)
            relay_half(COT, 1)
            along(B, "o", role)
            spread(B, "z")
            spread(B, "d")
            spread(B, "y")
            pass_near(COT)
            relay_on(A, "o", role)
            relay_on(A, "y", role)
            relay_on(A, "z", role)
            relay_on(A, "d", role)
        pass_far(EARLY)
        arrived(B, "z", role)
        relay_on(B, "o", role)
        pass_far(COT)

    def by_role(steps):
        @pl.when(is_inner)
        def _():
            steps(1)

        @pl.when(is_outer)
        def _():
            steps(0)

    for a in range(3):
        start("tc", a, OWN)
    local = [
        pltpu.make_async_copy(
            wt.at[seat("o"), g], w.at[g, :, :, lanes(zh, *seats["o"], x)], local_sems.at[g]
        )
        for g in range(n_parts)
    ]
    for copy in local:
        copy.start()
    by_role(take_in)
    for copy in local:
        copy.wait()
    weights_here(A)
    tokens_here(EARLY)
    tokens_here(COT)
    early(A)
    arrived(B, "d", 1)
    arrived(B, "y", 1)
    own_all(LATE)
    weight_grads(A)
    relay_on(B, "z", 1)
    relay_on(B, "d", 1)
    relay_on(B, "y", 1)
    grad_far(A)
    relay_tokens(LATE)
    pass_near(LATE)
    weights_here(B)
    early(B)
    partial_both(0, ((dgu, 2, GATE),))
    grad_relay(A, 0, 1)
    join_cores(0)
    weight_grads(B)
    grad_far(B)
    grad_near(A, 0, 1, 2, 3)
    grad_relay(A, 2, 3)
    pass_far(LATE)
    tokens_here(LATE)
    late()
    grad_relay(B, 0)
    partial_both(1, ((hidl, 1, DOWN),))
    grad_relay(B, 1)
    join_cores(1)
    grad_relay(B, 2, 3)
    grad_near(B, 0, 1, 2, 3)
    out_relay(0)
    out_relay(1)
    early_final()
    grad_final(A)
    grad_final(B)
    late_final()
    grad_done(A)
    grad_done(B)
    g_out[...] = gx[...]
    assert len(net.copies) == N_COPIES, len(net.copies)
    only_outer = [("ga", A, q) for q in "oyzd"]
    only_inner = [(n, A, q) for n in ("h", "gb", "gc") for q in "oyzd"]

    def drain(role):
        for name, copy in net.copies.items():
            if name in (only_inner if role else only_outer):
                copy.wait_send()

    for name, copy in net.copies.items():
        if name not in only_inner + only_outer:
            copy.wait_send()
    by_role(drain)


def run_step(wt, x_late, x_early, cotangent, norm_gain):
    _, n_parts, _, part, rows = wt.shape
    own, width = x_early.shape
    tokens = 2 * GROUP * own
    bf16 = jnp.bfloat16
    vmem = pltpu.VMEM
    return pl.pallas_call(
        step_kernel,
        out_shape=(
            jax.ShapeDtypeStruct((own, width), bf16),
            jax.ShapeDtypeStruct((own, width), bf16),
            jax.ShapeDtypeStruct((GROUP, n_parts, 3 * part, rows), bf16),
        ),
        in_specs=[pl.BlockSpec(memory_space=pltpu.VMEM)] * 5,
        out_specs=[pl.BlockSpec(memory_space=pltpu.VMEM)] * 3,
        scratch_shapes=[
            vmem((n_parts, 3, part, width), bf16),
            vmem((3, tokens, width), bf16),
            vmem((n_parts, part, tokens), bf16),
            vmem((n_parts, 2 * part, tokens), bf16),
            vmem((n_parts, part, tokens), bf16),
            vmem((n_parts, 2, 2, GROUP, 3 * part, rows), bf16),
            vmem((2, tokens, width), bf16),
            vmem((2, tokens // 2, width), bf16),
            vmem((2, 2, own // 2, width), bf16),
            vmem((2, 2, own, width), bf16),
            vmem((n_parts, GROUP, 3 * part, rows), bf16),
            vmem((n_parts, 2, GROUP, 3 * part, rows), bf16),
            vmem((n_parts, GROUP, 3 * part, rows), bf16),
            vmem((GROUP, n_parts, 3 * part, rows), bf16),
            vmem((GROUP, 3, part, rows), bf16),
            vmem((GROUP, 3, part, rows), bf16),
            pltpu.SemaphoreType.DMA((N_COPIES,)),
            pltpu.SemaphoreType.DMA((N_COPIES,)),
            pltpu.SemaphoreType.DMA((n_parts,)),
        ],
        compiler_params=pltpu.CompilerParams(
            collective_id=0, has_side_effects=True, vmem_limit_bytes=60 * 2**20
        ),
        name="step",
    )(wt, x_late, x_early, cotangent, norm_gain.reshape(1, -1))


def on_device_step(
    x_late, x_early, cotangent, norm_gain,
    gate_weight, up_weight, down_weight, gate_sum, up_sum, down_sum,
):
    rows, cols = gate_weight.shape
    stacked = jnp.stack([gate_weight, up_weight, down_weight])
    wt = stacked.reshape(3, rows, GROUP, PARTS, cols // (GROUP * PARTS))
    wt = wt.transpose(2, 3, 0, 4, 1)
    out_late, grad_early, grads = run_step(wt, x_late, x_early, cotangent, norm_gain)
    grads = grads.reshape(wt.shape).transpose(2, 4, 0, 1, 3)
    grads = grads.reshape(3, rows, cols).astype(jnp.float32)
    return (
        out_late,
        grad_early,
        gate_sum + grads[0],
        up_sum + grads[1],
        down_sum + grads[2],
    )


WANTED = 8


def solution(mesh):
    n_fs, n_tp = mesh.shape["fs"], mesh.shape["tp"]
    if n_tp == 2 and n_fs == 4 * GROUP:
        axes, body = ("zh", "zi", "y", "x", "tp"), on_device_step
        fine = Mesh(mesh.devices.reshape(2, 2, 2, 2, n_tp), axes)
    else:
        split = max(1, WANTED // n_tp)
        while n_fs % split:
            split //= 2
        axes, body = ("fo", "fi", "tp"), make_on_device(split, n_tp)
        fine = Mesh(mesh.devices.reshape(n_fs // split, split, n_tp), axes)
    tokens, rows = P(axes, None), P(axes[:-1], "tp")
    return jax.shard_map(
        body,
        mesh=fine,
        in_specs=(tokens, tokens, tokens, P()) + (rows,) * 6,
        out_specs=(tokens, tokens, rows, rows, rows),
        check_vma=False,
    )
```

```python
import jax
import jax.numpy as jnp
from jax import lax
from jax.experimental import pallas as pl
from jax.experimental.pallas import tpu as pltpu
from jax.sharding import Mesh
from jax.sharding import PartitionSpec as P

eps = 1e-06


def normalize(x, gain):
    xf = x.astype(jnp.float32)
    inv = lax.rsqrt(jnp.mean(xf * xf, axis=-1, keepdims=True) + eps)
    return (inv, (xf * inv * gain).astype(jnp.bfloat16))


def contract_last(left, right):
    return lax.dot_general(
        left, right, (((1,), (1,)), ((), ())), preferred_element_type=jnp.float32
    )


def contract_first(left, right):
    return lax.dot_general(
        left, right, (((0,), (0,)), ((), ())), preferred_element_type=jnp.float32
    )


def dot(left, right):
    return jnp.dot(left, right, preferred_element_type=jnp.float32)


def make_on_device(split, n_tp):
    def shifted(value, axis, size, step):
        return lax.ppermute(value, axis, [(i, (i + step) % size) for i in range(size)])

    def gather_tokens(own):
        over_fi = [own] + [shifted(own, "fi", split, k) for k in range(1, split)]
        chip = jnp.concatenate(over_fi, axis=1)
        over_tp = [chip] + [shifted(chip, "tp", n_tp, j) for j in range(1, n_tp)]
        return jnp.concatenate(over_tp, axis=1)

    def scatter_tokens(part):
        blocks = part.astype(jnp.bfloat16).reshape((n_tp, split, -1, part.shape[-1]))
        mine = blocks[0].astype(jnp.float32)
        for j in range(1, n_tp):
            mine = mine + shifted(blocks[j], "tp", n_tp, -j).astype(jnp.float32)
        total = mine[0]
        if split > 1:
            sent = mine[1:].astype(jnp.bfloat16)
            for k in range(1, split):
                total = total + shifted(sent[k - 1], "fi", split, -k).astype(jnp.float32)
        return total

    def gather_weight(parts):
        rows, cols = parts[0].shape
        width = cols // split
        if split > 1:
            pieces = [p.reshape(rows, split, width).transpose(1, 0, 2) for p in parts]
            sent = jnp.concatenate(pieces, axis=2) if len(pieces) > 1 else pieces[0]
            sent = lax.all_to_all(sent, "fi", split_axis=0, concat_axis=0, tiled=True)
            sent = sent.reshape(split * rows, len(parts) * width)
        else:
            sent = jnp.concatenate(parts, axis=1) if len(parts) > 1 else parts[0]
        return lax.all_gather(sent, "fo", axis=0, tiled=True)

    def scatter_grad(grad, sums):
        rows, cols = sums[0].shape
        width = cols // split
        part = lax.psum_scatter(
            grad.astype(jnp.bfloat16), "fo", scatter_dimension=0, tiled=True
        )
        part = part.reshape(split, rows, len(sums) * width)
        if split > 1:
            part = lax.all_to_all(part, "fi", split_axis=0, concat_axis=0, tiled=True)
        outs = []
        for i, s in enumerate(sums):
            own = part[:, :, i * width : (i + 1) * width]
            own = own.transpose(1, 0, 2).reshape(rows, cols)
            outs.append(s + own.astype(jnp.float32))
        return outs

    def on_device(
        x_late,
        x_early,
        cotangent,
        norm_gain,
        gate_weight,
        up_weight,
        down_weight,
        gate_sum,
        up_sum,
        down_sum,
    ):
        width = gate_weight.shape[1] // split
        gain = norm_gain.astype(jnp.float32)
        inv_own, early_own = normalize(x_early, gain)
        _, late_own = normalize(x_late, gain)
        cot_own = (0.5 * cotangent.astype(jnp.float32)).astype(jnp.bfloat16)
        w_gu = gather_weight([gate_weight, up_weight])
        early_side = gather_tokens(jnp.stack([early_own, cot_own]))
        normed_early, half_cot = early_side[0], early_side[1]
        normed_late = gather_tokens(late_own[None])[0]
        w_down = gather_weight([down_weight])

        gu_e = dot(normed_early, w_gu)
        gate_e, up_e = gu_e[:, :width], gu_e[:, width:]
        sig = jax.nn.sigmoid(gate_e)
        silu_e = gate_e * sig
        hidden_e = (silu_e * up_e).astype(jnp.bfloat16)
        down_part = contract_first(half_cot, hidden_e)
        gu_l = dot(normed_late, w_gu)
        hidden_l = (jax.nn.silu(gu_l[:, :width]) * gu_l[:, width:]).astype(jnp.bfloat16)

        d_hidden = dot(half_cot, w_down)
        d_gate = (d_hidden * up_e * sig * (1.0 + gate_e * (1.0 - sig))).astype(jnp.bfloat16)
        d_up = (d_hidden * silu_e).astype(jnp.bfloat16)
        d_gu = jnp.concatenate([d_gate, d_up], axis=1)
        gu_part = contract_first(normed_early, d_gu)

        (down_out,) = scatter_grad(down_part, [down_sum])
        gate_out, up_out = scatter_grad(gu_part, [gate_sum, up_sum])

        d_normed = scatter_tokens(contract_last(d_gu, w_gu))
        branch = scatter_tokens(contract_last(hidden_l, w_down))
        out_late = (x_late.astype(jnp.float32) + 0.5 * branch).astype(jnp.bfloat16)
        early_f = x_early.astype(jnp.float32)
        scaled = d_normed * gain
        d_input = inv_own * scaled - early_f * inv_own**3 * jnp.mean(
            scaled * early_f, axis=-1, keepdims=True
        )
        grad_early = (cotangent.astype(jnp.float32) + d_input).astype(jnp.bfloat16)
        return (out_late, grad_early, gate_out, up_out, down_out)

    return on_device


MESH = pl.DeviceIdType.MESH
PARTS = 2
GROUP = 4
EARLY, COT, LATE = 0, 1, 2
GATE, UP, DOWN = 0, 1, 2
OWN, ZN, YN, DIAG = 0, 1, 2, 3


def dot_nt(left, right):
    return lax.dot_general(
        left, right, (((1,), (1,)), ((), ())), preferred_element_type=jnp.float32
    )


def dot_tn(left, right):
    return lax.dot_general(
        left, right, (((0,), (0,)), ((), ())), preferred_element_type=jnp.float32
    )


class Net:
    def __init__(self, send_sems, recv_sems):
        self.send_sems, self.recv_sems, self.copies = send_sems, recv_sems, {}

    def plan(self, name, src, dst, device):
        i = len(self.copies)
        self.copies[name] = pltpu.make_async_remote_copy(
            src_ref=src,
            dst_ref=dst,
            send_sem=self.send_sems.at[i],
            recv_sem=self.recv_sems.at[i],
            device_id=device,
            device_id_type=MESH,
        )

    def start(self, *name):
        self.copies[name].start()

    def recv(self, *name):
        self.copies[name].wait_recv()


N_COPIES = 116


def step_kernel(
    gate_weight, up_weight, down_weight, x_late, x_early, cotangent, norm_gain,
    late_out, early_out, g_out,
    wt, w, tok, hid, dgu, hidl, gr, po, px_in, o_relay, o_dir, g_relay, g_dir, gs, gx,
    gwa, gwb, acc,
    send_sems, recv_sems, local_sems,
):
    _, n_parts, _, part, rows = wt.shape
    own_tokens, width = x_early.shape
    tokens = tok.shape[1]
    half = own_tokens // 2
    zh, zi = lax.axis_index("zh"), lax.axis_index("zi")
    y, x, c = lax.axis_index("y"), lax.axis_index("x"), lax.axis_index("tp")
    inner = lax.rem(zh + zi, 2)
    is_inner, is_outer = inner == 1, inner == 0
    to_x, to_y, to_z = {"x": 1 - x}, {"y": 1 - y}, {"zi": 1 - zi}
    to_d, to_c = {"zi": 1 - zi, "y": 1 - y}, {"tp": 1 - c}
    to_m = {"zh": 1 - zh, "zi": 1 - zi}

    barrier = pltpu.get_barrier_semaphore()
    partners = (to_x, to_y, to_z, to_d, to_m, to_c)
    for device in partners:
        pl.semaphore_signal(barrier, inc=1, device_id=device, device_id_type=MESH)

    def own_rows(a):
        return tok.at[a, pl.ds((GROUP + OWN) * own_tokens, own_tokens)]

    for m, weight in enumerate((gate_weight, up_weight, down_weight)):
        turned = weight[...].T
        for k in range(GROUP * n_parts):
            wt[k // n_parts, k % n_parts, m] = turned[k * part : (k + 1) * part]
    gain = norm_gain[...].astype(jnp.float32).reshape(1, width)
    own_rows(EARLY)[...] = normalize(x_early[...], gain)[1]
    own_rows(COT)[...] = (0.5 * cotangent[...].astype(jnp.float32)).astype(jnp.bfloat16)
    own_rows(LATE)[...] = normalize(x_late[...], gain)[1]
    pl.semaphore_wait(barrier, len(partners))

    net = Net(send_sems, recv_sems)
    start, recv, plan = net.start, net.recv, net.plan
    A, B = 0, 1
    seats = {"o": (inner, y), "y": (inner, 1 - y), "z": (1 - inner, y), "d": (1 - inner, 1 - y)}
    toward = {"y": to_y, "z": to_z, "d": to_d}

    def seat(q):
        return seats[q][0] * 2 + seats[q][1]

    def lanes(zh_, in_, y_, x_):
        z_ = in_ + zh_ * (3 - 2 * in_)
        return pl.ds(pl.multiple_of(((z_ * 2 + y_) * 2 + x_) * rows, rows), rows)

    def slot(rel, r=1):
        return pl.ds((r * GROUP + rel) * own_tokens, own_tokens)

    def half_slot(rel, h, r=1):
        return pl.ds((r * GROUP + rel) * own_tokens + h * half, half)

    for g in range(n_parts):
        for q in "yzd":
            plan(("a", g, q), wt.at[seat(q), g], w.at[g, :, :, lanes(zh, *seats["o"], x)], toward[q])
        for i, q in enumerate("oyzd"):
            block = w.at[g, :, :, lanes(zh, *seats[q], x)]
            src = wt.at[seat("o"), g] if q == "o" else block
            plan(("h", g, q), src, block, to_m)
            far = w.at[g, :, :, lanes(1 - zh, *seats[q], x)]
            if g == A:
                outer_seat = (1 - seats[q][0], seats[q][1])
                outer_far = w.at[g, :, :, lanes(1 - zh, *outer_seat, x)]
                plan(("ga", g, q), src, gwa.at[i], to_z)
                plan(("gb", g, q), gwa.at[i], gwb.at[i], to_m)
                plan(("gc", g, q), gwb.at[i], outer_far, to_z)
            plan(("x", g, q), src, block, to_x)
            plan(("xr", g, q), far, far, to_x)
        for k in range(GROUP):
            mine = gr.at[g, 1 - zh, x, k]
            plan(("gr", g, k), gr.at[g, 1 - zh, 1 - x, k], g_relay.at[g, k], to_x)
            plan(("gx", g, k), gr.at[g, zh, 1 - x, k], g_dir.at[g, 0, k], to_x)
            plan(("gh", g, k), mine, g_dir.at[g, 1, k], to_m)
        for q in "dzy":
            plan(("gf", g, q), gs.at[g, seat(q)], gx.at[seat("o"), g], toward[q])
    for a in range(3):
        for h in range(2):
            src = tok.at[a, half_slot(OWN, h)]
            plan(("tz", a, h), src, tok.at[a, half_slot(ZN, h)], to_z)
            plan(("ty", a, h), src, tok.at[a, half_slot(YN, h)], to_y)
            plan(("tr", a, h), tok.at[a, half_slot(ZN, h)], tok.at[a, half_slot(DIAG, h)], to_y)
        for rel in range(GROUP):
            plan(("tc", a, rel), tok.at[a, slot(rel)], tok.at[a, slot(rel, 0)], to_c)
    for a in range(2):
        plan(("oc", a), po.at[a, pl.ds(0, GROUP * own_tokens)], px_in.at[a], to_c)
        for h in range(2):
            to_half = o_dir.at[a, 0, pl.ds(h * half, half)]
            plan(("oy", a, h), po.at[a, half_slot(YN, h)], to_half, to_y)
            plan(("od", a, h), po.at[a, half_slot(DIAG, h)], o_relay.at[a, h], to_y)
            to_half = o_dir.at[a, 1, pl.ds(h * half, half)]
            plan(("oz", a, h), po.at[a, half_slot(ZN, h)], to_half, to_z)

    def spread(g, q):
        start("a", g, q)

    def along(g, q, role):
        start("ga" if g == A and not role else "h", g, q)
        start("x", g, q)

    def arrived(g, q, role):
        recv("a", g, q)
        along(g, q, role)

    def relay_on(g, q, role):
        recv("gc" if g == A and not role else "h", g, q)
        start("xr", g, q)

    def pass1(g, *some):
        for q in some:
            recv("ga", g, q)
            start("gb", g, q)

    def pass2(g, *some):
        for q in some:
            recv("gb", g, q)
            start("gc", g, q)

    def weights_here(g):
        for q in "oyzd":
            recv("x", g, q)
            recv("xr", g, q)

    def own_half(a, h):
        start("tz", a, h)
        start("ty", a, h)

    def own_all(a):
        own_half(a, 0)
        own_half(a, 1)

    def relay_half(a, h):
        recv("tz", a, h)
        start("tr", a, h)
        if h == 1:
            start("tc", a, ZN)

    def relay_tokens(a):
        relay_half(a, 0)
        relay_half(a, 1)

    def pass_near(a):
        for h in range(2):
            recv("ty", a, h)
        start("tc", a, YN)

    def pass_far(a):
        for h in range(2):
            recv("tr", a, h)
        start("tc", a, DIAG)

    def tokens_here(a):
        for rel in range(GROUP):
            recv("tc", a, rel)

    chunk = 2 * 128
    n_chunks = tokens // chunk
    span = 4 * rows
    group = tokens // 2

    def chunk_of(n):
        return pl.ds(pl.multiple_of(n * chunk, chunk), chunk)

    def span_of(n):
        return pl.ds(pl.multiple_of(n * span, span), span)

    def merged(ref):
        value = ref[...]
        return value.reshape(value.shape[0] * value.shape[1], value.shape[2])

    def gate_up(g, rows_in):
        both = dot_nt(merged(w.at[g, pl.ds(0, 2)]), rows_in)
        return both[:part], both[part:]

    def early(g):
        @pl.loop(0, n_chunks)
        def _(n):
            cols = chunk_of(n)
            gate, up = gate_up(g, tok[EARLY, cols, :])
            d_hidden = dot_nt(w[g, DOWN], tok[COT, cols, :])
            sig = jax.nn.sigmoid(gate)
            silu = gate * sig
            hid[g, :, cols] = (silu * up).astype(jnp.bfloat16)
            d_gate = d_hidden * up * sig * (1.0 + gate * (1.0 - sig))
            dgu[g, pl.ds(0, part), cols] = d_gate.astype(jnp.bfloat16)
            dgu[g, pl.ds(part, part), cols] = (d_hidden * silu).astype(jnp.bfloat16)

    def weight_grads(g):
        @pl.loop(0, width // span)
        def _(n):
            cols = span_of(n)
            for at, left, a in ((0, dgu, EARLY), (2 * part, hid, COT)):
                grad = jnp.dot(
                    left[g], tok[a, :, cols], preferred_element_type=jnp.float32
                ).astype(jnp.bfloat16)
                for yy in range(2):
                    for xx in range(2):
                        k = (yy * 2 + xx) * rows
                        gr[g, n // 2, xx, ((n + n // 2) % 2) * 2 + yy, pl.ds(at, grad.shape[0])] = (
                            grad[:, k : k + rows]
                        )

    def late(g):
        @pl.loop(0, n_chunks)
        def _(n):
            cols = chunk_of(n)
            gate, up = gate_up(g, tok[LATE, cols, :])
            hidl[g, :, cols] = (gate * jax.nn.sigmoid(gate) * up).astype(jnp.bfloat16)

    def add_to(ref, index, term):
        ref[index] = (ref[index].astype(jnp.float32) + term.astype(jnp.float32)).astype(
            jnp.bfloat16
        )

    def grad_far(g):
        for k in range(GROUP):
            start("gr", g, k)

    def grad_near(g, *some):
        for k in some:
            start("gx", g, k)

    def grad_relay(g, *some):
        for k in some:
            recv("gr", g, k)
            add_to(gr, (g, 1 - zh, x, k), g_relay[g, k])
            start("gh", g, k)

    def grad_final(g):
        for k in range(GROUP):
            recv("gh", g, k)
        for k in range(GROUP):
            recv("gx", g, k)
            total = gr[g, zh, x, k].astype(jnp.float32)
            total = total + g_dir[g, 0, k].astype(jnp.float32)
            total = total + g_dir[g, 1, k].astype(jnp.float32)
            gs[g, k] = total.astype(jnp.bfloat16)
        for q in "dzy":
            start("gf", g, q)
        gx[seat("o"), g] = gs[g, seat("o")]

    def grad_done(g):
        for q in "dzy":
            recv("gf", g, q)

    def term(g, r, ref, height, m, cols):
        left = ref[g, :, pl.ds(r * group, group)]
        return dot_tn(left, merged(w.at[g, pl.ds(m, height), :, cols]))

    def half_partial(ref, height, m):
        @pl.loop(0, width // span)
        def _(n):
            cols = span_of(n)
            for r in range(2):
                acc[pl.ds(r * group, group), cols] = term(A, r, ref, height, m, cols)

    def partial(a, r, ref, height, m):
        @pl.loop(0, width // span)
        def _(n):
            cols = span_of(n)
            at = pl.ds(r * group, group)
            total = acc[at, cols] + term(B, r, ref, height, m, cols)
            po[a, at, cols] = total.astype(jnp.bfloat16)

    def partial_both(a, *what):
        partial(a, 0, *what)
        start("oc", a)
        partial(a, 1, *what)

    def join_cores(a):
        recv("oc", a)

        @pl.loop(0, GROUP)
        def _(n):
            at = pl.ds(pl.multiple_of(n * own_tokens, own_tokens), own_tokens)
            at_po = pl.ds(pl.multiple_of(group + n * own_tokens, own_tokens), own_tokens)
            add_to(po, (a, at_po, slice(None)), px_in[a, at, :])

        for h in range(2):
            start("od", a, h)
        start("oy", 0, a)
        if a == 1:
            start("oy", 1, 0)
            start("oy", 1, 1)

    def out_relay(a):
        for h in range(2):
            recv("od", a, h)
            add_to(po, (a, half_slot(ZN, h), slice(None)), o_relay[a, h])
            start("oz", a, h)

    def out_total(a):
        for h in range(2):
            recv("oy", a, h)
            recv("oz", a, h)
        return (
            po[a, slot(OWN), :].astype(jnp.float32)
            + o_dir[a, 0].astype(jnp.float32)
            + o_dir[a, 1].astype(jnp.float32)
        )

    def early_final():
        early_f = x_early[...].astype(jnp.float32)
        inv = normalize(early_f, gain)[0]
        scaled = out_total(0) * gain
        d_input = inv * scaled - early_f * inv**3 * jnp.mean(
            scaled * early_f, axis=-1, keepdims=True
        )
        early_out[...] = (cotangent[...].astype(jnp.float32) + d_input).astype(jnp.bfloat16)

    def late_final():
        late_f = x_late[...].astype(jnp.float32)
        late_out[...] = (late_f + 0.5 * out_total(1)).astype(jnp.bfloat16)

    def take_in(role):
        for q in "zdy":
            spread(A, q)
        along(A, "o", role)
        own_half(EARLY, 0)
        if role:
            own_half(EARLY, 1)
        arrived(A, "y", role)
        arrived(A, "z", role)
        arrived(A, "d", role)
        if not role:
            own_half(EARLY, 1)
        for q in "zdy":
            spread(B, q)
        own_all(COT)
        if role:
            relay_on(A, "o", role)
            pass1(A, "o")
            relay_on(A, "y", role)
            relay_on(A, "z", role)
            relay_half(EARLY, 0)
            relay_on(A, "d", role)
            pass1(A, "y")
            pass2(A, "o")
            pass_near(EARLY)
            pass1(A, "z")
            pass2(A, "y")
            pass1(A, "d")
            along(B, "o", role)
            pass2(A, "z")
            arrived(B, "y", role)
            relay_half(EARLY, 1)
            pass2(A, "d")
            arrived(B, "z", role)
            pass_near(COT)
            arrived(B, "d", role)
            relay_half(COT, 0)
            relay_on(B, "o", role)
            relay_half(COT, 1)
        else:
            relay_half(EARLY, 0)
            relay_half(EARLY, 1)
            pass_near(EARLY)
            along(B, "o", role)
            arrived(B, "z", role)
            arrived(B, "y", role)
            arrived(B, "d", role)
            relay_half(COT, 0)
            relay_half(COT, 1)
            relay_on(A, "o", role)
            pass_near(COT)
            relay_on(A, "y", role)
            relay_on(A, "z", role)
            relay_on(A, "d", role)
            relay_on(B, "o", role)
        pass_far(EARLY)
        own_all(LATE)
        pass_far(COT)

    def by_role(steps):
        @pl.when(is_inner)
        def _():
            steps(1)

        @pl.when(is_outer)
        def _():
            steps(0)

    for a in range(3):
        start("tc", a, OWN)
    local = [
        pltpu.make_async_copy(
            wt.at[seat("o"), g], w.at[g, :, :, lanes(zh, *seats["o"], x)], local_sems.at[g]
        )
        for g in range(n_parts)
    ]
    for copy in local:
        copy.start()
    by_role(take_in)
    for copy in local:
        copy.wait()
    weights_here(A)
    tokens_here(EARLY)
    tokens_here(COT)
    early(A)
    relay_on(B, "y", 1)
    relay_on(B, "z", 1)
    weight_grads(A)
    relay_on(B, "d", 1)
    grad_far(A)
    grad_near(A, 0, 1)
    half_partial(dgu, 2, GATE)
    relay_tokens(LATE)
    pass_near(LATE)
    weights_here(B)
    early(B)
    partial_both(0, dgu, 2, GATE)
    grad_relay(A, 0, 1)
    weight_grads(B)
    grad_far(B)
    grad_near(A, 2, 3)
    join_cores(0)
    grad_relay(A, 2, 3)
    pass_far(LATE)
    tokens_here(LATE)
    late(A)
    half_partial(hidl, 1, DOWN)
    late(B)
    partial_both(1, hidl, 1, DOWN)
    out_relay(0)
    grad_relay(B, 0)
    join_cores(1)
    grad_relay(B, 1, 2, 3)
    grad_near(B, 0, 1, 2, 3)
    out_relay(1)
    grad_final(A)
    early_final()
    grad_final(B)
    late_final()
    grad_done(A)
    grad_done(B)
    for m in range(3):
        blocks = [
            gx[k // n_parts, k % n_parts, pl.ds(m * part, part)]
            for k in range(GROUP * n_parts)
        ]
        g_out[m] = jnp.concatenate(blocks, axis=0).T
    assert len(net.copies) == N_COPIES, len(net.copies)
    only_outer = [("ga", A, q) for q in "oyzd"]
    only_inner = [(n, A, q) for n in ("h", "gb", "gc") for q in "oyzd"]

    def drain(role):
        for name, copy in net.copies.items():
            if name in (only_inner if role else only_outer):
                copy.wait_send()

    for name, copy in net.copies.items():
        if name not in only_inner + only_outer:
            copy.wait_send()
    by_role(drain)


def run_step(gate_weight, up_weight, down_weight, x_late, x_early, cotangent, norm_gain):
    rows, cols = gate_weight.shape
    n_parts, part = PARTS, cols // (GROUP * PARTS)
    own, width = x_early.shape
    tokens = 2 * GROUP * own
    bf16 = jnp.bfloat16
    vmem = pltpu.VMEM
    return pl.pallas_call(
        step_kernel,
        out_shape=(
            jax.ShapeDtypeStruct((own, width), bf16),
            jax.ShapeDtypeStruct((own, width), bf16),
            jax.ShapeDtypeStruct((3, rows, cols), bf16),
        ),
        in_specs=[pl.BlockSpec(memory_space=pltpu.VMEM)] * 7,
        out_specs=[pl.BlockSpec(memory_space=pltpu.VMEM)] * 3,
        scratch_shapes=[
            vmem((GROUP, n_parts, 3, part, rows), bf16),
            vmem((n_parts, 3, part, width), bf16),
            vmem((3, tokens, width), bf16),
            vmem((n_parts, part, tokens), bf16),
            vmem((n_parts, 2 * part, tokens), bf16),
            vmem((n_parts, part, tokens), bf16),
            vmem((n_parts, 2, 2, GROUP, 3 * part, rows), bf16),
            vmem((2, tokens, width), bf16),
            vmem((2, tokens // 2, width), bf16),
            vmem((2, 2, own // 2, width), bf16),
            vmem((2, 2, own, width), bf16),
            vmem((n_parts, GROUP, 3 * part, rows), bf16),
            vmem((n_parts, 2, GROUP, 3 * part, rows), bf16),
            vmem((n_parts, GROUP, 3 * part, rows), bf16),
            vmem((GROUP, n_parts, 3 * part, rows), bf16),
            vmem((GROUP, 3, part, rows), bf16),
            vmem((GROUP, 3, part, rows), bf16),
            vmem((tokens, width), jnp.float32),
            pltpu.SemaphoreType.DMA((N_COPIES,)),
            pltpu.SemaphoreType.DMA((N_COPIES,)),
            pltpu.SemaphoreType.DMA((n_parts,)),
        ],
        compiler_params=pltpu.CompilerParams(
            collective_id=0, has_side_effects=True, vmem_limit_bytes=60 * 2**20
        ),
        name="step",
    )(gate_weight, up_weight, down_weight, x_late, x_early, cotangent, norm_gain)


def on_device_step(
    x_late, x_early, cotangent, norm_gain,
    gate_weight, up_weight, down_weight, gate_sum, up_sum, down_sum,
):
    out_late, grad_early, grads = run_step(
        gate_weight, up_weight, down_weight, x_late, x_early, cotangent, norm_gain
    )
    sums = (gate_sum, up_sum, down_sum)
    outs = [s + grads[m].astype(jnp.float32) for m, s in enumerate(sums)]
    return (out_late, grad_early, *outs)


WANTED = 8


def solution(mesh):
    n_fs, n_tp = mesh.shape["fs"], mesh.shape["tp"]
    if n_tp == 2 and n_fs == 4 * GROUP:
        axes, body = ("zh", "zi", "y", "x", "tp"), on_device_step
        fine = Mesh(mesh.devices.reshape(2, 2, 2, 2, n_tp), axes)
    else:
        split = max(1, WANTED // n_tp)
        while n_fs % split:
            split //= 2
        axes, body = ("fo", "fi", "tp"), make_on_device(split, n_tp)
        fine = Mesh(mesh.devices.reshape(n_fs // split, split, n_tp), axes)
    tokens, rows = P(axes, None), P(axes[:-1], "tp")
    return jax.shard_map(
        body,
        mesh=fine,
        in_specs=(tokens, tokens, tokens, P()) + (rows,) * 6,
        out_specs=(tokens, tokens, rows, rows, rows),
        check_vma=False,
    )
```

```python
import jax
import jax.numpy as jnp
from jax import lax
from jax.experimental import pallas as pl
from jax.experimental.pallas import tpu as pltpu
from jax.sharding import Mesh
from jax.sharding import PartitionSpec as P

eps = 1e-06


def normalize(x, gain):
    xf = x.astype(jnp.float32)
    inv = lax.rsqrt(jnp.mean(xf * xf, axis=-1, keepdims=True) + eps)
    return (inv, (xf * inv * gain).astype(jnp.bfloat16))


def contract_last(left, right):
    return lax.dot_general(
        left, right, (((1,), (1,)), ((), ())), preferred_element_type=jnp.float32
    )


def contract_first(left, right):
    return lax.dot_general(
        left, right, (((0,), (0,)), ((), ())), preferred_element_type=jnp.float32
    )


def dot(left, right):
    return jnp.dot(left, right, preferred_element_type=jnp.float32)


def make_on_device(split, n_tp):
    def shifted(value, axis, size, step):
        return lax.ppermute(value, axis, [(i, (i + step) % size) for i in range(size)])

    def gather_tokens(own):
        over_fi = [own] + [shifted(own, "fi", split, k) for k in range(1, split)]
        chip = jnp.concatenate(over_fi, axis=1)
        over_tp = [chip] + [shifted(chip, "tp", n_tp, j) for j in range(1, n_tp)]
        return jnp.concatenate(over_tp, axis=1)

    def scatter_tokens(part):
        blocks = part.astype(jnp.bfloat16).reshape((n_tp, split, -1, part.shape[-1]))
        mine = blocks[0].astype(jnp.float32)
        for j in range(1, n_tp):
            mine = mine + shifted(blocks[j], "tp", n_tp, -j).astype(jnp.float32)
        total = mine[0]
        if split > 1:
            sent = mine[1:].astype(jnp.bfloat16)
            for k in range(1, split):
                total = total + shifted(sent[k - 1], "fi", split, -k).astype(jnp.float32)
        return total

    def gather_weight(parts):
        rows, cols = parts[0].shape
        width = cols // split
        if split > 1:
            pieces = [p.reshape(rows, split, width).transpose(1, 0, 2) for p in parts]
            sent = jnp.concatenate(pieces, axis=2) if len(pieces) > 1 else pieces[0]
            sent = lax.all_to_all(sent, "fi", split_axis=0, concat_axis=0, tiled=True)
            sent = sent.reshape(split * rows, len(parts) * width)
        else:
            sent = jnp.concatenate(parts, axis=1) if len(parts) > 1 else parts[0]
        return lax.all_gather(sent, "fo", axis=0, tiled=True)

    def scatter_grad(grad, sums):
        rows, cols = sums[0].shape
        width = cols // split
        part = lax.psum_scatter(
            grad.astype(jnp.bfloat16), "fo", scatter_dimension=0, tiled=True
        )
        part = part.reshape(split, rows, len(sums) * width)
        if split > 1:
            part = lax.all_to_all(part, "fi", split_axis=0, concat_axis=0, tiled=True)
        outs = []
        for i, s in enumerate(sums):
            own = part[:, :, i * width : (i + 1) * width]
            own = own.transpose(1, 0, 2).reshape(rows, cols)
            outs.append(s + own.astype(jnp.float32))
        return outs

    def on_device(
        x_late,
        x_early,
        cotangent,
        norm_gain,
        gate_weight,
        up_weight,
        down_weight,
        gate_sum,
        up_sum,
        down_sum,
    ):
        width = gate_weight.shape[1] // split
        gain = norm_gain.astype(jnp.float32)
        inv_own, early_own = normalize(x_early, gain)
        _, late_own = normalize(x_late, gain)
        cot_own = (0.5 * cotangent.astype(jnp.float32)).astype(jnp.bfloat16)
        w_gu = gather_weight([gate_weight, up_weight])
        early_side = gather_tokens(jnp.stack([early_own, cot_own]))
        normed_early, half_cot = early_side[0], early_side[1]
        normed_late = gather_tokens(late_own[None])[0]
        w_down = gather_weight([down_weight])

        gu_e = dot(normed_early, w_gu)
        gate_e, up_e = gu_e[:, :width], gu_e[:, width:]
        sig = jax.nn.sigmoid(gate_e)
        silu_e = gate_e * sig
        hidden_e = (silu_e * up_e).astype(jnp.bfloat16)
        down_part = contract_first(half_cot, hidden_e)
        gu_l = dot(normed_late, w_gu)
        hidden_l = (jax.nn.silu(gu_l[:, :width]) * gu_l[:, width:]).astype(jnp.bfloat16)

        d_hidden = dot(half_cot, w_down)
        d_gate = (d_hidden * up_e * sig * (1.0 + gate_e * (1.0 - sig))).astype(jnp.bfloat16)
        d_up = (d_hidden * silu_e).astype(jnp.bfloat16)
        d_gu = jnp.concatenate([d_gate, d_up], axis=1)
        gu_part = contract_first(normed_early, d_gu)

        (down_out,) = scatter_grad(down_part, [down_sum])
        gate_out, up_out = scatter_grad(gu_part, [gate_sum, up_sum])

        d_normed = scatter_tokens(contract_last(d_gu, w_gu))
        branch = scatter_tokens(contract_last(hidden_l, w_down))
        out_late = (x_late.astype(jnp.float32) + 0.5 * branch).astype(jnp.bfloat16)
        early_f = x_early.astype(jnp.float32)
        scaled = d_normed * gain
        d_input = inv_own * scaled - early_f * inv_own**3 * jnp.mean(
            scaled * early_f, axis=-1, keepdims=True
        )
        grad_early = (cotangent.astype(jnp.float32) + d_input).astype(jnp.bfloat16)
        return (out_late, grad_early, gate_out, up_out, down_out)

    return on_device


MESH = pl.DeviceIdType.MESH
PARTS = 2
GROUP = 4
EARLY, COT, LATE = 0, 1, 2
GATE, UP, DOWN = 0, 1, 2
OWN, ZN, YN, DIAG = 0, 1, 2, 3


def dot_nt(left, right):
    return lax.dot_general(
        left, right, (((1,), (1,)), ((), ())), preferred_element_type=jnp.float32
    )


def dot_tn(left, right):
    return lax.dot_general(
        left, right, (((0,), (0,)), ((), ())), preferred_element_type=jnp.float32
    )


class Net:
    def __init__(self, send_sems, recv_sems):
        self.send_sems, self.recv_sems, self.copies = send_sems, recv_sems, {}

    def plan(self, name, src, dst, device):
        i = len(self.copies)
        self.copies[name] = pltpu.make_async_remote_copy(
            src_ref=src,
            dst_ref=dst,
            send_sem=self.send_sems.at[i],
            recv_sem=self.recv_sems.at[i],
            device_id=device,
            device_id_type=MESH,
        )

    def start(self, *name):
        self.copies[name].start()

    def recv(self, *name):
        self.copies[name].wait_recv()


N_COPIES = 116


def step_kernel(
    gate_weight, up_weight, down_weight, x_late, x_early, cotangent, norm_gain,
    late_out, early_out, g_out,
    wt, w, tok, hid, dgu, hidl, gr, po, px_in, o_relay, o_dir, g_relay, g_dir, gs, gx,
    gwa, gwb, acc, early_own, late_own, g_own,
    send_sems, recv_sems, local_sems,
):
    _, n_parts, _, part, rows = wt.shape
    own_tokens, width = x_early.shape
    tokens = tok.shape[1]
    half = own_tokens // 2
    zh, zi = lax.axis_index("zh"), lax.axis_index("zi")
    y, x, c = lax.axis_index("y"), lax.axis_index("x"), lax.axis_index("tp")
    inner = lax.rem(zh + zi, 2)
    is_inner, is_outer = inner == 1, inner == 0
    to_x, to_y, to_z = {"x": 1 - x}, {"y": 1 - y}, {"zi": 1 - zi}
    to_d, to_c = {"zi": 1 - zi, "y": 1 - y}, {"tp": 1 - c}
    to_m = {"zh": 1 - zh, "zi": 1 - zi}

    barrier = pltpu.get_barrier_semaphore()
    partners = (to_x, to_y, to_z, to_d, to_m, to_c)
    for device in partners:
        pl.semaphore_signal(barrier, inc=1, device_id=device, device_id_type=MESH)

    def own_rows(a):
        return tok.at[a, pl.ds((GROUP + OWN) * own_tokens, own_tokens)]

    def turn_in(g):
        lo, hi = g * GROUP * part, (g + 1) * GROUP * part
        lo_at, hi_at = lo // 128 * 128, -(-hi // 128) * 128
        for m, weight in enumerate((gate_weight, up_weight, down_weight)):
            turned = weight[:, lo_at:hi_at].T
            for k in range(GROUP):
                at = lo - lo_at + k * part
                wt[k, g, m] = turned[at : at + part]

    turn_in(0)
    gain = norm_gain[...].astype(jnp.float32).reshape(1, width)
    pl.semaphore_wait(barrier, len(partners))

    net = Net(send_sems, recv_sems)
    start, recv, plan = net.start, net.recv, net.plan
    A, B = 0, 1
    seats = {"o": (inner, y), "y": (inner, 1 - y), "z": (1 - inner, y), "d": (1 - inner, 1 - y)}
    toward = {"y": to_y, "z": to_z, "d": to_d}

    def seat(q):
        return seats[q][0] * 2 + seats[q][1]

    def lanes(zh_, in_, y_, x_):
        z_ = in_ + zh_ * (3 - 2 * in_)
        return pl.ds(pl.multiple_of(((z_ * 2 + y_) * 2 + x_) * rows, rows), rows)

    def slot(rel, r=1):
        return pl.ds((r * GROUP + rel) * own_tokens, own_tokens)

    def half_slot(rel, h, r=1):
        return pl.ds((r * GROUP + rel) * own_tokens + h * half, half)

    for g in range(n_parts):
        for q in "yzd":
            plan(("a", g, q), wt.at[seat(q), g], w.at[g, :, :, lanes(zh, *seats["o"], x)], toward[q])
        for i, q in enumerate("oyzd"):
            block = w.at[g, :, :, lanes(zh, *seats[q], x)]
            src = wt.at[seat("o"), g] if q == "o" else block
            plan(("h", g, q), src, block, to_m)
            far = w.at[g, :, :, lanes(1 - zh, *seats[q], x)]
            if g == A:
                outer_seat = (1 - seats[q][0], seats[q][1])
                outer_far = w.at[g, :, :, lanes(1 - zh, *outer_seat, x)]
                plan(("ga", g, q), src, gwa.at[i], to_z)
                plan(("gb", g, q), gwa.at[i], gwb.at[i], to_m)
                plan(("gc", g, q), gwb.at[i], outer_far, to_z)
            plan(("x", g, q), src, block, to_x)
            plan(("xr", g, q), far, far, to_x)
        for k in range(GROUP):
            mine = gr.at[g, 1 - zh, x, k]
            plan(("gr", g, k), gr.at[g, 1 - zh, 1 - x, k], g_relay.at[g, k], to_x)
            plan(("gx", g, k), gr.at[g, zh, 1 - x, k], g_dir.at[g, 0, k], to_x)
            plan(("gh", g, k), mine, g_dir.at[g, 1, k], to_m)
        for q in "dzy":
            plan(("gf", g, q), gs.at[g, seat(q)], gx.at[seat("o"), g], toward[q])
    for a in range(3):
        for h in range(2):
            src = tok.at[a, half_slot(OWN, h)]
            plan(("tz", a, h), src, tok.at[a, half_slot(ZN, h)], to_z)
            plan(("ty", a, h), src, tok.at[a, half_slot(YN, h)], to_y)
            plan(("tr", a, h), tok.at[a, half_slot(ZN, h)], tok.at[a, half_slot(DIAG, h)], to_y)
        for rel in range(GROUP):
            plan(("tc", a, rel), tok.at[a, slot(rel)], tok.at[a, slot(rel, 0)], to_c)
    for a in range(2):
        plan(("oc", a), po.at[a, pl.ds(0, GROUP * own_tokens)], px_in.at[a], to_c)
        for h in range(2):
            to_half = o_dir.at[a, 0, pl.ds(h * half, half)]
            plan(("oy", a, h), po.at[a, half_slot(YN, h)], to_half, to_y)
            plan(("od", a, h), po.at[a, half_slot(DIAG, h)], o_relay.at[a, h], to_y)
            to_half = o_dir.at[a, 1, pl.ds(h * half, half)]
            plan(("oz", a, h), po.at[a, half_slot(ZN, h)], to_half, to_z)

    def spread(g, q):
        start("a", g, q)

    def along(g, q, role):
        start("ga" if g == A and not role else "h", g, q)
        start("x", g, q)

    def arrived(g, q, role):
        recv("a", g, q)
        along(g, q, role)

    def relay_on(g, q, role):
        recv("gc" if g == A and not role else "h", g, q)
        start("xr", g, q)

    def pass1(g, *some):
        for q in some:
            recv("ga", g, q)
            start("gb", g, q)

    def pass2(g, *some):
        for q in some:
            recv("gb", g, q)
            start("gc", g, q)

    def weights_here(g):
        for q in "oyzd":
            recv("x", g, q)
            recv("xr", g, q)

    def own_half(a, h):
        start("tz", a, h)
        start("ty", a, h)

    def own_all(a):
        own_half(a, 0)
        own_half(a, 1)

    def relay_half(a, h):
        recv("tz", a, h)
        start("tr", a, h)
        if h == 1:
            start("tc", a, ZN)

    def relay_tokens(a):
        relay_half(a, 0)
        relay_half(a, 1)

    def pass_near(a):
        for h in range(2):
            recv("ty", a, h)
        start("tc", a, YN)

    def pass_far(a):
        for h in range(2):
            recv("tr", a, h)
        start("tc", a, DIAG)

    def tokens_here(a):
        for rel in range(GROUP):
            recv("tc", a, rel)

    chunk = 2 * 128
    n_chunks = tokens // chunk
    span = 4 * rows
    group = tokens // 2

    def chunk_of(n):
        return pl.ds(pl.multiple_of(n * chunk, chunk), chunk)

    def span_of(n):
        return pl.ds(pl.multiple_of(n * span, span), span)

    def merged(ref):
        value = ref[...]
        return value.reshape(value.shape[0] * value.shape[1], value.shape[2])

    def gate_up(g, rows_in):
        both = dot_nt(merged(w.at[g, pl.ds(0, 2)]), rows_in)
        return both[:part], both[part:]

    def early(g, lo=0, hi=n_chunks):
        @pl.loop(lo, hi)
        def _(n):
            cols = chunk_of(n)
            gate, up = gate_up(g, tok[EARLY, cols, :])
            d_hidden = dot_nt(w[g, DOWN], tok[COT, cols, :])
            sig = jax.nn.sigmoid(gate)
            silu = gate * sig
            hid[g, :, cols] = (silu * up).astype(jnp.bfloat16)
            d_gate = d_hidden * up * sig * (1.0 + gate * (1.0 - sig))
            dgu[g, pl.ds(0, part), cols] = d_gate.astype(jnp.bfloat16)
            dgu[g, pl.ds(part, part), cols] = (d_hidden * silu).astype(jnp.bfloat16)

    def weight_grads(g):
        @pl.loop(0, width // span)
        def _(n):
            cols = span_of(n)
            for at, left, a in ((0, dgu, EARLY), (2 * part, hid, COT)):
                grad = jnp.dot(
                    left[g], tok[a, :, cols], preferred_element_type=jnp.float32
                ).astype(jnp.bfloat16)
                for yy in range(2):
                    for xx in range(2):
                        k = (yy * 2 + xx) * rows
                        gr[g, n // 2, xx, ((n + n // 2) % 2) * 2 + yy, pl.ds(at, grad.shape[0])] = (
                            grad[:, k : k + rows]
                        )

    def late(g, lo=0, hi=n_chunks):
        @pl.loop(lo, hi)
        def _(n):
            cols = chunk_of(n)
            gate, up = gate_up(g, tok[LATE, cols, :])
            hidl[g, :, cols] = (gate * jax.nn.sigmoid(gate) * up).astype(jnp.bfloat16)

    def add_to(ref, index, term):
        ref[index] = (ref[index].astype(jnp.float32) + term.astype(jnp.float32)).astype(
            jnp.bfloat16
        )

    def grad_far(g):
        for k in range(GROUP):
            start("gr", g, k)

    def grad_near(g, *some):
        for k in some:
            start("gx", g, k)

    def grad_relay(g, *some):
        for k in some:
            recv("gr", g, k)
            add_to(gr, (g, 1 - zh, x, k), g_relay[g, k])
            start("gh", g, k)

    def grad_final(g):
        for k in range(GROUP):
            recv("gh", g, k)
        for k in range(GROUP):
            recv("gx", g, k)
            total = gr[g, zh, x, k].astype(jnp.float32)
            total = total + g_dir[g, 0, k].astype(jnp.float32)
            total = total + g_dir[g, 1, k].astype(jnp.float32)
            gs[g, k] = total.astype(jnp.bfloat16)
        for q in "dzy":
            start("gf", g, q)
        gx[seat("o"), g] = gs[g, seat("o")]

    def grad_done(g):
        for q in "dzy":
            recv("gf", g, q)

    def term(g, r, ref, height, m, cols):
        left = ref[g, :, pl.ds(r * group, group)]
        return dot_tn(left, merged(w.at[g, pl.ds(m, height), :, cols]))

    def half_partial(ref, height, m):
        @pl.loop(0, width // span)
        def _(n):
            cols = span_of(n)
            for r in range(2):
                acc[pl.ds(r * group, group), cols] = term(A, r, ref, height, m, cols)

    def partial(a, r, ref, height, m):
        @pl.loop(0, width // span)
        def _(n):
            cols = span_of(n)
            at = pl.ds(r * group, group)
            total = acc[at, cols] + term(B, r, ref, height, m, cols)
            po[a, at, cols] = total.astype(jnp.bfloat16)

    ahead = -(-group // chunk)

    def partial_both(a, step, *what):
        step(B, 0, ahead)
        partial(a, 0, *what)
        start("oc", a)
        step(B, ahead, n_chunks)
        partial(a, 1, *what)

    def join_cores(a):
        recv("oc", a)

        @pl.loop(0, GROUP)
        def _(n):
            at = pl.ds(pl.multiple_of(n * own_tokens, own_tokens), own_tokens)
            at_po = pl.ds(pl.multiple_of(group + n * own_tokens, own_tokens), own_tokens)
            add_to(po, (a, at_po, slice(None)), px_in[a, at, :])

        for h in range(2):
            start("od", a, h)
        start("oy", 0, a)
        if a == 1:
            start("oy", 1, 0)
            start("oy", 1, 1)

    def out_relay(a):
        for h in range(2):
            recv("od", a, h)
            add_to(po, (a, half_slot(ZN, h), slice(None)), o_relay[a, h])
            start("oz", a, h)

    def out_total(a):
        for h in range(2):
            recv("oy", a, h)
            recv("oz", a, h)
        return (
            po[a, slot(OWN), :].astype(jnp.float32)
            + o_dir[a, 0].astype(jnp.float32)
            + o_dir[a, 1].astype(jnp.float32)
        )

    def early_final():
        early_f = x_early[...].astype(jnp.float32)
        inv = normalize(early_f, gain)[0]
        scaled = out_total(0) * gain
        d_input = inv * scaled - early_f * inv**3 * jnp.mean(
            scaled * early_f, axis=-1, keepdims=True
        )
        early_own[...] = (cotangent[...].astype(jnp.float32) + d_input).astype(jnp.bfloat16)
        to_hbm[3].start()

    def late_final():
        late_f = x_late[...].astype(jnp.float32)
        late_own[...] = (late_f + 0.5 * out_total(1)).astype(jnp.bfloat16)
        to_hbm[4].start()

    to_hbm = [
        pltpu.make_async_copy(g_own.at[m], g_out.at[m], local_sems.at[n_parts + m])
        for m in range(3)
    ]
    to_hbm.append(pltpu.make_async_copy(early_own, early_out, local_sems.at[n_parts + 3]))
    to_hbm.append(pltpu.make_async_copy(late_own, late_out, local_sems.at[n_parts + 4]))

    def take_in(role):
        own_half(EARLY, 0)
        if role:
            own_half(EARLY, 1)
        arrived(A, "y", role)
        arrived(A, "z", role)
        arrived(A, "d", role)
        if not role:
            own_half(EARLY, 1)
        for q in "zdy":
            spread(B, q)
        own_all(COT)
        if role:
            relay_on(A, "o", role)
            pass1(A, "o")
            relay_on(A, "y", role)
            relay_on(A, "z", role)
            relay_half(EARLY, 0)
            relay_on(A, "d", role)
            pass1(A, "y")
            pass2(A, "o")
            pass_near(EARLY)
            pass1(A, "z")
            pass2(A, "y")
            pass1(A, "d")
            along(B, "o", role)
            pass2(A, "z")
            arrived(B, "y", role)
            relay_half(EARLY, 1)
            pass2(A, "d")
            arrived(B, "z", role)
            pass_near(COT)
            arrived(B, "d", role)
            relay_half(COT, 0)
            relay_on(B, "o", role)
            relay_half(COT, 1)
        else:
            relay_half(EARLY, 0)
            relay_half(EARLY, 1)
            pass_near(EARLY)
            along(B, "o", role)
            arrived(B, "z", role)
            arrived(B, "y", role)
            arrived(B, "d", role)
            relay_half(COT, 0)
            relay_half(COT, 1)
            relay_on(A, "o", role)
            pass_near(COT)
            relay_on(A, "y", role)
            relay_on(A, "z", role)
            relay_on(A, "d", role)
            relay_on(B, "o", role)
        pass_far(EARLY)
        own_all(LATE)
        pass_far(COT)

    def by_role(steps):
        @pl.when(is_inner)
        def _():
            steps(1)

        @pl.when(is_outer)
        def _():
            steps(0)

    for q in "zdy":
        spread(A, q)
    by_role(lambda role: along(A, "o", role))
    own_rows(EARLY)[...] = normalize(x_early[...], gain)[1]
    half_cot = 0.5 * cotangent[...].astype(jnp.float32)
    own_rows(COT)[...] = half_cot.astype(jnp.bfloat16)
    own_rows(LATE)[...] = normalize(x_late[...], gain)[1]
    for g in range(1, n_parts):
        turn_in(g)
    for a in range(3):
        start("tc", a, OWN)
    local = [
        pltpu.make_async_copy(
            wt.at[seat("o"), g], w.at[g, :, :, lanes(zh, *seats["o"], x)], local_sems.at[g]
        )
        for g in range(n_parts)
    ]
    for copy in local:
        copy.start()
    by_role(take_in)
    for copy in local:
        copy.wait()
    weights_here(A)
    tokens_here(EARLY)
    tokens_here(COT)
    early(A)
    relay_on(B, "y", 1)
    relay_on(B, "z", 1)
    weight_grads(A)
    relay_on(B, "d", 1)
    grad_far(A)
    grad_near(A, 0, 1)
    half_partial(dgu, 2, GATE)
    relay_tokens(LATE)
    pass_near(LATE)
    weights_here(B)
    partial_both(0, early, dgu, 2, GATE)
    pass_far(LATE)
    grad_relay(A, 0, 1)
    join_cores(0)
    weight_grads(B)
    grad_far(B)
    grad_near(A, 2, 3)
    grad_relay(A, 2, 3)
    tokens_here(LATE)
    late(A)
    half_partial(hidl, 1, DOWN)
    partial_both(1, late, hidl, 1, DOWN)
    out_relay(0)
    grad_relay(B, 0)
    join_cores(1)
    grad_relay(B, 1, 2, 3)
    grad_near(B, 0, 1, 2, 3)
    out_relay(1)
    grad_final(A)
    early_final()
    grad_final(B)
    late_final()
    at_row = lax.broadcasted_iota(jnp.int32, (rows, rows), 0)
    at_column = lax.broadcasted_iota(jnp.int32, (rows, rows), 1)
    eye = jnp.where(at_row == at_column, 1.0, 0.0).astype(jnp.bfloat16)
    def turn(m, lo, hi):
        blocks = []
        for k in range(lo // part, -(-hi // part)):
            first, last = max(lo - k * part, 0), min(hi - k * part, part)
            at = pl.ds(m * part + first, last - first)
            blocks.append(gx[k % GROUP, k // GROUP, at])
        turned = dot_nt(eye, jnp.concatenate(blocks, axis=0))
        g_own[m, :, pl.ds(lo, hi - lo)] = turned.astype(jnp.bfloat16)

    columns = n_parts * GROUP * part
    early_columns = GROUP * part // 128 * 128
    grad_done(A)
    for m in range(3):
        turn(m, 0, early_columns)
    grad_done(B)
    for m in range(3):
        turn(m, early_columns, columns)
        to_hbm[m].start()
    for copy in to_hbm:
        copy.wait()
    assert len(net.copies) == N_COPIES, len(net.copies)
    only_outer = [("ga", A, q) for q in "oyzd"]
    only_inner = [(n, A, q) for n in ("h", "gb", "gc") for q in "oyzd"]

    def drain(role):
        for name, copy in net.copies.items():
            if name in (only_inner if role else only_outer):
                copy.wait_send()

    for name, copy in net.copies.items():
        if name not in only_inner + only_outer:
            copy.wait_send()
    by_role(drain)


def run_step(gate_weight, up_weight, down_weight, x_late, x_early, cotangent, norm_gain):
    rows, cols = gate_weight.shape
    n_parts, part = PARTS, cols // (GROUP * PARTS)
    own, width = x_early.shape
    tokens = 2 * GROUP * own
    bf16 = jnp.bfloat16
    vmem = pltpu.VMEM
    return pl.pallas_call(
        step_kernel,
        out_shape=(
            jax.ShapeDtypeStruct((own, width), bf16),
            jax.ShapeDtypeStruct((own, width), bf16),
            jax.ShapeDtypeStruct((3, rows, cols), bf16),
        ),
        in_specs=[pl.BlockSpec(memory_space=pltpu.VMEM)] * 7,
        out_specs=[pl.BlockSpec(memory_space=pl.ANY)] * 3,
        scratch_shapes=[
            vmem((GROUP, n_parts, 3, part, rows), bf16),
            vmem((n_parts, 3, part, width), bf16),
            vmem((3, tokens, width), bf16),
            vmem((n_parts, part, tokens), bf16),
            vmem((n_parts, 2 * part, tokens), bf16),
            vmem((n_parts, part, tokens), bf16),
            vmem((n_parts, 2, 2, GROUP, 3 * part, rows), bf16),
            vmem((2, tokens, width), bf16),
            vmem((2, tokens // 2, width), bf16),
            vmem((2, 2, own // 2, width), bf16),
            vmem((2, 2, own, width), bf16),
            vmem((n_parts, GROUP, 3 * part, rows), bf16),
            vmem((n_parts, 2, GROUP, 3 * part, rows), bf16),
            vmem((n_parts, GROUP, 3 * part, rows), bf16),
            vmem((GROUP, n_parts, 3 * part, rows), bf16),
            vmem((GROUP, 3, part, rows), bf16),
            vmem((GROUP, 3, part, rows), bf16),
            vmem((tokens, width), jnp.float32),
            vmem((own, width), bf16),
            vmem((own, width), bf16),
            vmem((3, rows, cols), bf16),
            pltpu.SemaphoreType.DMA((N_COPIES,)),
            pltpu.SemaphoreType.DMA((N_COPIES,)),
            pltpu.SemaphoreType.DMA((n_parts + 5,)),
        ],
        compiler_params=pltpu.CompilerParams(
            collective_id=0, has_side_effects=True, vmem_limit_bytes=60 * 2**20
        ),
        name="step",
    )(gate_weight, up_weight, down_weight, x_late, x_early, cotangent, norm_gain)


def on_device_step(
    x_late, x_early, cotangent, norm_gain,
    gate_weight, up_weight, down_weight, gate_sum, up_sum, down_sum,
):
    out_late, grad_early, grads = run_step(
        gate_weight, up_weight, down_weight, x_late, x_early, cotangent, norm_gain
    )
    sums = (gate_sum, up_sum, down_sum)
    outs = [s + grads[m].astype(jnp.float32) for m, s in enumerate(sums)]
    return (out_late, grad_early, *outs)


WANTED = 8


def solution(mesh):
    n_fs, n_tp = mesh.shape["fs"], mesh.shape["tp"]
    if n_tp == 2 and n_fs == 4 * GROUP:
        axes, body = ("zh", "zi", "y", "x", "tp"), on_device_step
        fine = Mesh(mesh.devices.reshape(2, 2, 2, 2, n_tp), axes)
    else:
        split = max(1, WANTED // n_tp)
        while n_fs % split:
            split //= 2
        axes, body = ("fo", "fi", "tp"), make_on_device(split, n_tp)
        fine = Mesh(mesh.devices.reshape(n_fs // split, split, n_tp), axes)
    tokens, rows = P(axes, None), P(axes[:-1], "tp")
    return jax.shard_map(
        body,
        mesh=fine,
        in_specs=(tokens, tokens, tokens, P()) + (rows,) * 6,
        out_specs=(tokens, tokens, rows, rows, rows),
        check_vma=False,
    )
```

```python
import jax
import jax.numpy as jnp
from jax import lax
from jax.experimental import pallas as pl
from jax.experimental.pallas import tpu as pltpu
from jax.sharding import Mesh
from jax.sharding import PartitionSpec as P

eps = 1e-06


def normalize(x, gain):
    xf = x.astype(jnp.float32)
    inv = lax.rsqrt(jnp.mean(xf * xf, axis=-1, keepdims=True) + eps)
    return (inv, (xf * inv * gain).astype(jnp.bfloat16))


def contract_last(left, right):
    return lax.dot_general(
        left, right, (((1,), (1,)), ((), ())), preferred_element_type=jnp.float32
    )


def contract_first(left, right):
    return lax.dot_general(
        left, right, (((0,), (0,)), ((), ())), preferred_element_type=jnp.float32
    )


def dot(left, right):
    return jnp.dot(left, right, preferred_element_type=jnp.float32)


def make_on_device(split, n_tp):
    def shifted(value, axis, size, step):
        return lax.ppermute(value, axis, [(i, (i + step) % size) for i in range(size)])

    def gather_tokens(own):
        over_fi = [own] + [shifted(own, "fi", split, k) for k in range(1, split)]
        chip = jnp.concatenate(over_fi, axis=1)
        over_tp = [chip] + [shifted(chip, "tp", n_tp, j) for j in range(1, n_tp)]
        return jnp.concatenate(over_tp, axis=1)

    def scatter_tokens(part):
        blocks = part.astype(jnp.bfloat16).reshape((n_tp, split, -1, part.shape[-1]))
        mine = blocks[0].astype(jnp.float32)
        for j in range(1, n_tp):
            mine = mine + shifted(blocks[j], "tp", n_tp, -j).astype(jnp.float32)
        total = mine[0]
        if split > 1:
            sent = mine[1:].astype(jnp.bfloat16)
            for k in range(1, split):
                total = total + shifted(sent[k - 1], "fi", split, -k).astype(jnp.float32)
        return total

    def gather_weight(parts):
        rows, cols = parts[0].shape
        width = cols // split
        if split > 1:
            pieces = [p.reshape(rows, split, width).transpose(1, 0, 2) for p in parts]
            sent = jnp.concatenate(pieces, axis=2) if len(pieces) > 1 else pieces[0]
            sent = lax.all_to_all(sent, "fi", split_axis=0, concat_axis=0, tiled=True)
            sent = sent.reshape(split * rows, len(parts) * width)
        else:
            sent = jnp.concatenate(parts, axis=1) if len(parts) > 1 else parts[0]
        return lax.all_gather(sent, "fo", axis=0, tiled=True)

    def scatter_grad(grad, sums):
        rows, cols = sums[0].shape
        width = cols // split
        part = lax.psum_scatter(
            grad.astype(jnp.bfloat16), "fo", scatter_dimension=0, tiled=True
        )
        part = part.reshape(split, rows, len(sums) * width)
        if split > 1:
            part = lax.all_to_all(part, "fi", split_axis=0, concat_axis=0, tiled=True)
        outs = []
        for i, s in enumerate(sums):
            own = part[:, :, i * width : (i + 1) * width]
            own = own.transpose(1, 0, 2).reshape(rows, cols)
            outs.append(s + own.astype(jnp.float32))
        return outs

    def on_device(
        x_late,
        x_early,
        cotangent,
        norm_gain,
        gate_weight,
        up_weight,
        down_weight,
        gate_sum,
        up_sum,
        down_sum,
    ):
        width = gate_weight.shape[1] // split
        gain = norm_gain.astype(jnp.float32)
        inv_own, early_own = normalize(x_early, gain)
        _, late_own = normalize(x_late, gain)
        cot_own = (0.5 * cotangent.astype(jnp.float32)).astype(jnp.bfloat16)
        w_gu = gather_weight([gate_weight, up_weight])
        early_side = gather_tokens(jnp.stack([early_own, cot_own]))
        normed_early, half_cot = early_side[0], early_side[1]
        normed_late = gather_tokens(late_own[None])[0]
        w_down = gather_weight([down_weight])

        gu_e = dot(normed_early, w_gu)
        gate_e, up_e = gu_e[:, :width], gu_e[:, width:]
        sig = jax.nn.sigmoid(gate_e)
        silu_e = gate_e * sig
        hidden_e = (silu_e * up_e).astype(jnp.bfloat16)
        down_part = contract_first(half_cot, hidden_e)
        gu_l = dot(normed_late, w_gu)
        hidden_l = (jax.nn.silu(gu_l[:, :width]) * gu_l[:, width:]).astype(jnp.bfloat16)

        d_hidden = dot(half_cot, w_down)
        d_gate = (d_hidden * up_e * sig * (1.0 + gate_e * (1.0 - sig))).astype(jnp.bfloat16)
        d_up = (d_hidden * silu_e).astype(jnp.bfloat16)
        d_gu = jnp.concatenate([d_gate, d_up], axis=1)
        gu_part = contract_first(normed_early, d_gu)

        (down_out,) = scatter_grad(down_part, [down_sum])
        gate_out, up_out = scatter_grad(gu_part, [gate_sum, up_sum])

        d_normed = scatter_tokens(contract_last(d_gu, w_gu))
        branch = scatter_tokens(contract_last(hidden_l, w_down))
        out_late = (x_late.astype(jnp.float32) + 0.5 * branch).astype(jnp.bfloat16)
        early_f = x_early.astype(jnp.float32)
        scaled = d_normed * gain
        d_input = inv_own * scaled - early_f * inv_own**3 * jnp.mean(
            scaled * early_f, axis=-1, keepdims=True
        )
        grad_early = (cotangent.astype(jnp.float32) + d_input).astype(jnp.bfloat16)
        return (out_late, grad_early, gate_out, up_out, down_out)

    return on_device


MESH = pl.DeviceIdType.MESH
PARTS = 2
GROUP = 4
EARLY, COT, LATE = 0, 1, 2
GATE, UP, DOWN = 0, 1, 2
OWN, ZN, YN, DIAG = 0, 1, 2, 3


def dot_nt(left, right):
    return lax.dot_general(
        left, right, (((1,), (1,)), ((), ())), preferred_element_type=jnp.float32
    )


def dot_tn(left, right):
    return lax.dot_general(
        left, right, (((0,), (0,)), ((), ())), preferred_element_type=jnp.float32
    )


class Net:
    def __init__(self, send_sems, recv_sems):
        self.send_sems, self.recv_sems, self.copies = send_sems, recv_sems, {}

    def plan(self, name, src, dst, device):
        i = len(self.copies)
        self.copies[name] = pltpu.make_async_remote_copy(
            src_ref=src,
            dst_ref=dst,
            send_sem=self.send_sems.at[i],
            recv_sem=self.recv_sems.at[i],
            device_id=device,
            device_id_type=MESH,
        )

    def start(self, *name):
        self.copies[name].start()

    def recv(self, *name):
        self.copies[name].wait_recv()


N_COPIES = 116


def step_kernel(
    gate_weight, up_weight, down_weight, x_late, x_early, cotangent, norm_gain,
    late_out, early_out, g_out,
    wt, w, tok, hid, dgu, hidl, gr, po, px_in, o_relay, o_dir, g_relay, g_dir, gs, gx,
    gwa, gwb, acc, early_in, cot_in, late_in, early_own, late_own, g_own,
    send_sems, recv_sems, local_sems,
):
    _, n_parts, _, part, rows = wt.shape
    own_tokens, width = x_early.shape
    tokens = tok.shape[1]
    half = own_tokens // 2
    zh, zi = lax.axis_index("zh"), lax.axis_index("zi")
    y, x, c = lax.axis_index("y"), lax.axis_index("x"), lax.axis_index("tp")
    inner = lax.rem(zh + zi, 2)
    is_inner, is_outer = inner == 1, inner == 0
    to_x, to_y, to_z = {"x": 1 - x}, {"y": 1 - y}, {"zi": 1 - zi}
    to_d, to_c = {"zi": 1 - zi, "y": 1 - y}, {"tp": 1 - c}
    to_m = {"zh": 1 - zh, "zi": 1 - zi}

    barrier = pltpu.get_barrier_semaphore()
    partners = (to_x, to_y, to_z, to_d, to_m, to_c)
    for device in partners:
        pl.semaphore_signal(barrier, inc=1, device_id=device, device_id_type=MESH)

    def own_rows(a):
        return tok.at[a, pl.ds((GROUP + OWN) * own_tokens, own_tokens)]

    inputs = [
        pltpu.make_async_copy(ref, own, local_sems.at[n_parts + 5 + i])
        for i, (ref, own) in enumerate(
            ((x_early, early_in), (cotangent, cot_in), (x_late, late_in))
        )
    ]
    for copy in inputs:
        copy.start()

    def turn_in(g):
        lo, hi = g * GROUP * part, (g + 1) * GROUP * part
        lo_at, hi_at = lo // 128 * 128, -(-hi // 128) * 128
        for m, weight in enumerate((gate_weight, up_weight, down_weight)):
            turned = weight[:, lo_at:hi_at].T
            for k in range(GROUP):
                at = lo - lo_at + k * part
                wt[k, g, m] = turned[at : at + part]

    turn_in(0)
    gain = norm_gain[...].astype(jnp.float32).reshape(1, width)
    pl.semaphore_wait(barrier, len(partners))

    net = Net(send_sems, recv_sems)
    start, recv, plan = net.start, net.recv, net.plan
    A, B = 0, 1
    seats = {"o": (inner, y), "y": (inner, 1 - y), "z": (1 - inner, y), "d": (1 - inner, 1 - y)}
    toward = {"y": to_y, "z": to_z, "d": to_d}

    def seat(q):
        return seats[q][0] * 2 + seats[q][1]

    def lanes(zh_, in_, y_, x_):
        z_ = in_ + zh_ * (3 - 2 * in_)
        return pl.ds(pl.multiple_of(((z_ * 2 + y_) * 2 + x_) * rows, rows), rows)

    def slot(rel, r=1):
        return pl.ds((r * GROUP + rel) * own_tokens, own_tokens)

    def half_slot(rel, h, r=1):
        return pl.ds((r * GROUP + rel) * own_tokens + h * half, half)

    for g in range(n_parts):
        for q in "yzd":
            plan(("a", g, q), wt.at[seat(q), g], w.at[g, :, :, lanes(zh, *seats["o"], x)], toward[q])
        for i, q in enumerate("oyzd"):
            block = w.at[g, :, :, lanes(zh, *seats[q], x)]
            src = wt.at[seat("o"), g] if q == "o" else block
            plan(("h", g, q), src, block, to_m)
            far = w.at[g, :, :, lanes(1 - zh, *seats[q], x)]
            if g == A:
                outer_seat = (1 - seats[q][0], seats[q][1])
                outer_far = w.at[g, :, :, lanes(1 - zh, *outer_seat, x)]
                plan(("ga", g, q), src, gwa.at[i], to_z)
                plan(("gb", g, q), gwa.at[i], gwb.at[i], to_m)
                plan(("gc", g, q), gwb.at[i], outer_far, to_z)
            plan(("x", g, q), src, block, to_x)
            plan(("xr", g, q), far, far, to_x)
        for k in range(GROUP):
            mine = gr.at[g, 1 - zh, x, k]
            plan(("gr", g, k), gr.at[g, 1 - zh, 1 - x, k], g_relay.at[g, k], to_x)
            plan(("gx", g, k), gr.at[g, zh, 1 - x, k], g_dir.at[g, 0, k], to_x)
            plan(("gh", g, k), mine, g_dir.at[g, 1, k], to_m)
        for q in "dzy":
            plan(("gf", g, q), gs.at[g, seat(q)], gx.at[seat("o"), g], toward[q])
    for a in range(3):
        for h in range(2):
            src = tok.at[a, half_slot(OWN, h)]
            plan(("tz", a, h), src, tok.at[a, half_slot(ZN, h)], to_z)
            plan(("ty", a, h), src, tok.at[a, half_slot(YN, h)], to_y)
            plan(("tr", a, h), tok.at[a, half_slot(ZN, h)], tok.at[a, half_slot(DIAG, h)], to_y)
        for rel in range(GROUP):
            plan(("tc", a, rel), tok.at[a, slot(rel)], tok.at[a, slot(rel, 0)], to_c)
    for a in range(2):
        plan(("oc", a), po.at[a, pl.ds(0, GROUP * own_tokens)], px_in.at[a], to_c)
        for h in range(2):
            to_half = o_dir.at[a, 0, pl.ds(h * half, half)]
            plan(("oy", a, h), po.at[a, half_slot(YN, h)], to_half, to_y)
            plan(("od", a, h), po.at[a, half_slot(DIAG, h)], o_relay.at[a, h], to_y)
            to_half = o_dir.at[a, 1, pl.ds(h * half, half)]
            plan(("oz", a, h), po.at[a, half_slot(ZN, h)], to_half, to_z)

    def spread(g, q):
        start("a", g, q)

    def along(g, q, role):
        start("ga" if g == A and not role else "h", g, q)
        start("x", g, q)

    def arrived(g, q, role):
        recv("a", g, q)
        along(g, q, role)

    def relay_on(g, q, role):
        recv("gc" if g == A and not role else "h", g, q)
        start("xr", g, q)

    def pass1(g, *some):
        for q in some:
            recv("ga", g, q)
            start("gb", g, q)

    def pass2(g, *some):
        for q in some:
            recv("gb", g, q)
            start("gc", g, q)

    def weights_here(g):
        for q in "oyzd":
            recv("x", g, q)
            recv("xr", g, q)

    def own_half(a, h):
        start("tz", a, h)
        start("ty", a, h)

    def own_all(a):
        own_half(a, 0)
        own_half(a, 1)

    def relay_half(a, h):
        recv("tz", a, h)
        start("tr", a, h)
        if h == 1:
            start("tc", a, ZN)

    def relay_tokens(a):
        relay_half(a, 0)
        relay_half(a, 1)

    def pass_near(a):
        for h in range(2):
            recv("ty", a, h)
        start("tc", a, YN)

    def pass_far(a):
        for h in range(2):
            recv("tr", a, h)
        start("tc", a, DIAG)

    def tokens_here(a):
        for rel in range(GROUP):
            recv("tc", a, rel)

    chunk = 2 * 128
    n_chunks = tokens // chunk
    span = 4 * rows
    group = tokens // 2

    def chunk_of(n):
        return pl.ds(pl.multiple_of(n * chunk, chunk), chunk)

    def span_of(n):
        return pl.ds(pl.multiple_of(n * span, span), span)

    def merged(ref):
        value = ref[...]
        return value.reshape(value.shape[0] * value.shape[1], value.shape[2])

    def gate_up(g, rows_in):
        both = dot_nt(merged(w.at[g, pl.ds(0, 2)]), rows_in)
        return both[:part], both[part:]

    def early(g, lo=0, hi=n_chunks):
        @pl.loop(lo, hi)
        def _(n):
            cols = chunk_of(n)
            gate, up = gate_up(g, tok[EARLY, cols, :])
            d_hidden = dot_nt(w[g, DOWN], tok[COT, cols, :])
            sig = jax.nn.sigmoid(gate)
            silu = gate * sig
            hid[g, :, cols] = (silu * up).astype(jnp.bfloat16)
            d_gate = d_hidden * up * sig * (1.0 + gate * (1.0 - sig))
            dgu[g, pl.ds(0, part), cols] = d_gate.astype(jnp.bfloat16)
            dgu[g, pl.ds(part, part), cols] = (d_hidden * silu).astype(jnp.bfloat16)

    def weight_grads(g):
        @pl.loop(0, width // span)
        def _(n):
            cols = span_of(n)
            for at, left, a in ((0, dgu, EARLY), (2 * part, hid, COT)):
                grad = jnp.dot(
                    left[g], tok[a, :, cols], preferred_element_type=jnp.float32
                ).astype(jnp.bfloat16)
                for yy in range(2):
                    for xx in range(2):
                        k = (yy * 2 + xx) * rows
                        gr[g, n // 2, xx, ((n + n // 2) % 2) * 2 + yy, pl.ds(at, grad.shape[0])] = (
                            grad[:, k : k + rows]
                        )

    def late(g, lo=0, hi=n_chunks):
        @pl.loop(lo, hi)
        def _(n):
            cols = chunk_of(n)
            gate, up = gate_up(g, tok[LATE, cols, :])
            hidl[g, :, cols] = (gate * jax.nn.sigmoid(gate) * up).astype(jnp.bfloat16)

    def add_to(ref, index, term):
        ref[index] = (ref[index].astype(jnp.float32) + term.astype(jnp.float32)).astype(
            jnp.bfloat16
        )

    def grad_far(g):
        for k in range(GROUP):
            start("gr", g, k)

    def grad_near(g, *some):
        for k in some:
            start("gx", g, k)

    def grad_relay(g, *some):
        for k in some:
            recv("gr", g, k)
            add_to(gr, (g, 1 - zh, x, k), g_relay[g, k])
            start("gh", g, k)

    def grad_final(g):
        for k in range(GROUP):
            recv("gh", g, k)
        for k in range(GROUP):
            recv("gx", g, k)
            total = gr[g, zh, x, k].astype(jnp.float32)
            total = total + g_dir[g, 0, k].astype(jnp.float32)
            total = total + g_dir[g, 1, k].astype(jnp.float32)
            gs[g, k] = total.astype(jnp.bfloat16)
        for q in "dzy":
            start("gf", g, q)
        gx[seat("o"), g] = gs[g, seat("o")]

    def grad_done(g):
        for q in "dzy":
            recv("gf", g, q)

    def term(g, r, ref, height, m, cols):
        left = ref[g, :, pl.ds(r * group, group)]
        return dot_tn(left, merged(w.at[g, pl.ds(m, height), :, cols]))

    def half_partial(ref, height, m):
        @pl.loop(0, width // span)
        def _(n):
            cols = span_of(n)
            for r in range(2):
                acc[pl.ds(r * group, group), cols] = term(A, r, ref, height, m, cols)

    def partial(a, r, ref, height, m):
        @pl.loop(0, width // span)
        def _(n):
            cols = span_of(n)
            at = pl.ds(r * group, group)
            total = acc[at, cols] + term(B, r, ref, height, m, cols)
            po[a, at, cols] = total.astype(jnp.bfloat16)

    ahead = -(-group // chunk)

    def partial_both(a, step, *what):
        step(B, 0, ahead)
        partial(a, 0, *what)
        start("oc", a)
        if a == 0:
            grad_relay(A, 0)
        step(B, ahead, n_chunks)
        partial(a, 1, *what)

    def join_cores(a):
        recv("oc", a)

        @pl.loop(0, GROUP)
        def _(n):
            at = pl.ds(pl.multiple_of(n * own_tokens, own_tokens), own_tokens)
            at_po = pl.ds(pl.multiple_of(group + n * own_tokens, own_tokens), own_tokens)
            add_to(po, (a, at_po, slice(None)), px_in[a, at, :])

        for h in range(2):
            start("od", a, h)
        start("oy", 0, a)
        if a == 1:
            start("oy", 1, 0)
            start("oy", 1, 1)

    def out_relay(a):
        for h in range(2):
            recv("od", a, h)
            add_to(po, (a, half_slot(ZN, h), slice(None)), o_relay[a, h])
            start("oz", a, h)

    def out_total(a):
        for h in range(2):
            recv("oy", a, h)
            recv("oz", a, h)
        return (
            po[a, slot(OWN), :].astype(jnp.float32)
            + o_dir[a, 0].astype(jnp.float32)
            + o_dir[a, 1].astype(jnp.float32)
        )

    def early_final():
        early_f = early_in[...].astype(jnp.float32)
        inv = normalize(early_f, gain)[0]
        scaled = out_total(0) * gain
        d_input = inv * scaled - early_f * inv**3 * jnp.mean(
            scaled * early_f, axis=-1, keepdims=True
        )
        early_own[...] = (cot_in[...].astype(jnp.float32) + d_input).astype(jnp.bfloat16)
        to_hbm[3].start()

    def late_final():
        late_f = late_in[...].astype(jnp.float32)
        late_own[...] = (late_f + 0.5 * out_total(1)).astype(jnp.bfloat16)
        to_hbm[4].start()

    to_hbm = [
        pltpu.make_async_copy(g_own.at[m], g_out.at[m], local_sems.at[n_parts + m])
        for m in range(3)
    ]
    to_hbm.append(pltpu.make_async_copy(early_own, early_out, local_sems.at[n_parts + 3]))
    to_hbm.append(pltpu.make_async_copy(late_own, late_out, local_sems.at[n_parts + 4]))

    def take_in(role):
        own_half(EARLY, 0)
        if role:
            own_half(EARLY, 1)
        arrived(A, "y", role)
        arrived(A, "z", role)
        arrived(A, "d", role)
        if not role:
            own_half(EARLY, 1)
        for q in "zdy":
            spread(B, q)
        own_all(COT)
        if role:
            relay_on(A, "o", role)
            pass1(A, "o")
            relay_on(A, "y", role)
            relay_on(A, "z", role)
            relay_half(EARLY, 0)
            relay_on(A, "d", role)
            pass1(A, "y")
            pass2(A, "o")
            pass_near(EARLY)
            pass1(A, "z")
            pass2(A, "y")
            pass1(A, "d")
            along(B, "o", role)
            pass2(A, "z")
            arrived(B, "y", role)
            relay_half(EARLY, 1)
            pass2(A, "d")
            arrived(B, "z", role)
            pass_near(COT)
            arrived(B, "d", role)
            relay_half(COT, 0)
            relay_on(B, "o", role)
            relay_half(COT, 1)
        else:
            relay_half(EARLY, 0)
            relay_half(EARLY, 1)
            pass_near(EARLY)
            along(B, "o", role)
            arrived(B, "z", role)
            arrived(B, "y", role)
            arrived(B, "d", role)
            relay_half(COT, 0)
            relay_half(COT, 1)
            relay_on(A, "o", role)
            pass_near(COT)
            relay_on(A, "y", role)
            relay_on(A, "z", role)
            relay_on(A, "d", role)
            relay_on(B, "o", role)
        pass_far(EARLY)
        own_all(LATE)
        pass_far(COT)

    def by_role(steps):
        @pl.when(is_inner)
        def _():
            steps(1)

        @pl.when(is_outer)
        def _():
            steps(0)

    for q in "zdy":
        spread(A, q)
    by_role(lambda role: along(A, "o", role))
    for copy in inputs:
        copy.wait()
    own_rows(EARLY)[...] = normalize(early_in[...], gain)[1]
    half_cot = 0.5 * cot_in[...].astype(jnp.float32)
    own_rows(COT)[...] = half_cot.astype(jnp.bfloat16)
    own_rows(LATE)[...] = normalize(late_in[...], gain)[1]
    for g in range(1, n_parts):
        turn_in(g)
    for a in range(3):
        start("tc", a, OWN)
    local = [
        pltpu.make_async_copy(
            wt.at[seat("o"), g], w.at[g, :, :, lanes(zh, *seats["o"], x)], local_sems.at[g]
        )
        for g in range(n_parts)
    ]
    for copy in local:
        copy.start()
    by_role(take_in)
    for copy in local:
        copy.wait()
    weights_here(A)
    tokens_here(EARLY)
    tokens_here(COT)
    early(A)
    relay_on(B, "y", 1)
    relay_on(B, "z", 1)
    weight_grads(A)
    relay_on(B, "d", 1)
    grad_far(A)
    grad_near(A, 0, 1)
    half_partial(dgu, 2, GATE)
    relay_tokens(LATE)
    pass_near(LATE)
    weights_here(B)
    partial_both(0, early, dgu, 2, GATE)
    pass_far(LATE)
    grad_relay(A, 1)
    join_cores(0)
    weight_grads(B)
    grad_far(B)
    grad_near(A, 2, 3)
    grad_relay(A, 2, 3)
    tokens_here(LATE)
    late(A)
    half_partial(hidl, 1, DOWN)
    partial_both(1, late, hidl, 1, DOWN)
    out_relay(0)
    grad_relay(B, 0)
    join_cores(1)
    grad_relay(B, 1, 2, 3)
    grad_near(B, 0, 1, 2, 3)
    out_relay(1)
    grad_final(A)
    early_final()
    grad_final(B)
    late_final()
    at_row = lax.broadcasted_iota(jnp.int32, (rows, rows), 0)
    at_column = lax.broadcasted_iota(jnp.int32, (rows, rows), 1)
    eye = jnp.where(at_row == at_column, 1.0, 0.0).astype(jnp.bfloat16)
    def turn(m, lo, hi):
        blocks = []
        for k in range(lo // part, -(-hi // part)):
            first, last = max(lo - k * part, 0), min(hi - k * part, part)
            at = pl.ds(m * part + first, last - first)
            blocks.append(gx[k % GROUP, k // GROUP, at])
        turned = dot_nt(eye, jnp.concatenate(blocks, axis=0))
        g_own[m, :, pl.ds(lo, hi - lo)] = turned.astype(jnp.bfloat16)

    columns = n_parts * GROUP * part
    early_columns = GROUP * part // 128 * 128
    grad_done(A)
    for m in range(3):
        turn(m, 0, early_columns)
    grad_done(B)
    for m in range(3):
        turn(m, early_columns, columns)
        to_hbm[m].start()
    for copy in to_hbm:
        copy.wait()
    assert len(net.copies) == N_COPIES, len(net.copies)
    only_outer = [("ga", A, q) for q in "oyzd"]
    only_inner = [(n, A, q) for n in ("h", "gb", "gc") for q in "oyzd"]

    def drain(role):
        for name, copy in net.copies.items():
            if name in (only_inner if role else only_outer):
                copy.wait_send()

    for name, copy in net.copies.items():
        if name not in only_inner + only_outer:
            copy.wait_send()
    by_role(drain)


def run_step(gate_weight, up_weight, down_weight, x_late, x_early, cotangent, norm_gain):
    rows, cols = gate_weight.shape
    n_parts, part = PARTS, cols // (GROUP * PARTS)
    own, width = x_early.shape
    tokens = 2 * GROUP * own
    bf16 = jnp.bfloat16
    vmem = pltpu.VMEM
    return pl.pallas_call(
        step_kernel,
        out_shape=(
            jax.ShapeDtypeStruct((own, width), bf16),
            jax.ShapeDtypeStruct((own, width), bf16),
            jax.ShapeDtypeStruct((3, rows, cols), bf16),
        ),
        in_specs=[pl.BlockSpec(memory_space=pltpu.VMEM)] * 3
        + [pl.BlockSpec(memory_space=pl.ANY)] * 3
        + [pl.BlockSpec(memory_space=pltpu.VMEM)],
        out_specs=[pl.BlockSpec(memory_space=pl.ANY)] * 3,
        scratch_shapes=[
            vmem((GROUP, n_parts, 3, part, rows), bf16),
            vmem((n_parts, 3, part, width), bf16),
            vmem((3, tokens, width), bf16),
            vmem((n_parts, part, tokens), bf16),
            vmem((n_parts, 2 * part, tokens), bf16),
            vmem((n_parts, part, tokens), bf16),
            vmem((n_parts, 2, 2, GROUP, 3 * part, rows), bf16),
            vmem((2, tokens, width), bf16),
            vmem((2, tokens // 2, width), bf16),
            vmem((2, 2, own // 2, width), bf16),
            vmem((2, 2, own, width), bf16),
            vmem((n_parts, GROUP, 3 * part, rows), bf16),
            vmem((n_parts, 2, GROUP, 3 * part, rows), bf16),
            vmem((n_parts, GROUP, 3 * part, rows), bf16),
            vmem((GROUP, n_parts, 3 * part, rows), bf16),
            vmem((GROUP, 3, part, rows), bf16),
            vmem((GROUP, 3, part, rows), bf16),
            vmem((tokens, width), jnp.float32),
            vmem((own, width), bf16),
            vmem((own, width), bf16),
            vmem((own, width), bf16),
            vmem((own, width), bf16),
            vmem((own, width), bf16),
            vmem((3, rows, cols), bf16),
            pltpu.SemaphoreType.DMA((N_COPIES,)),
            pltpu.SemaphoreType.DMA((N_COPIES,)),
            pltpu.SemaphoreType.DMA((n_parts + 8,)),
        ],
        compiler_params=pltpu.CompilerParams(
            collective_id=0, has_side_effects=True, vmem_limit_bytes=60 * 2**20
        ),
        name="step",
    )(gate_weight, up_weight, down_weight, x_late, x_early, cotangent, norm_gain)


def on_device_step(
    x_late, x_early, cotangent, norm_gain,
    gate_weight, up_weight, down_weight, gate_sum, up_sum, down_sum,
):
    out_late, grad_early, grads = run_step(
        gate_weight, up_weight, down_weight, x_late, x_early, cotangent, norm_gain
    )
    sums = (gate_sum, up_sum, down_sum)
    outs = [s + grads[m].astype(jnp.float32) for m, s in enumerate(sums)]
    return (out_late, grad_early, *outs)


WANTED = 8


def solution(mesh):
    n_fs, n_tp = mesh.shape["fs"], mesh.shape["tp"]
    if n_tp == 2 and n_fs == 4 * GROUP:
        axes, body = ("zh", "zi", "y", "x", "tp"), on_device_step
        fine = Mesh(mesh.devices.reshape(2, 2, 2, 2, n_tp), axes)
    else:
        split = max(1, WANTED // n_tp)
        while n_fs % split:
            split //= 2
        axes, body = ("fo", "fi", "tp"), make_on_device(split, n_tp)
        fine = Mesh(mesh.devices.reshape(n_fs // split, split, n_tp), axes)
    tokens, rows = P(axes, None), P(axes[:-1], "tp")
    return jax.shard_map(
        body,
        mesh=fine,
        in_specs=(tokens, tokens, tokens, P()) + (rows,) * 6,
        out_specs=(tokens, tokens, rows, rows, rows),
        check_vma=False,
    )
```
